256 devices in a mesh: sp: 64 (over z, x, core), tp: 4 (over y).
Axes of the slice: x: 4, y: 4, z: 8, core: 2. Of those that a mesh axis runs over, the one named last changes fastest.
Arguments:
- tokens: bfloat16 [8192, 2048], P('sp', 'tp'), may hold values from -6 to 6
- norm_gain: float32 [2048], replicated, may hold values from 0.1 to 1.9
- da_query: bfloat16 [2048, 1024], P(None, 'tp'), as said below
- da_key: bfloat16 [2048, 1024], P(None, 'tp'), may hold values from -0.125 to 0.125
- da_value: bfloat16 [2048, 1024], P(None, 'tp'), may hold values from -0.125 to 0.125
- mix_lambda: float32 [8], P('tp'), may hold values from 0.3 to 0.8
- attn_gain: float32 [128], replicated, may hold values from 0.1 to 1.9
- rec_query: bfloat16 [2048, 1024], P(None, 'tp'), may hold values from -0.125 to 0.125
- rec_forget_fwd: bfloat16 [2048, 1024], P(None, 'tp'), may hold values from -0.375 to 0.375
- rec_forget_bwd: bfloat16 [2048, 1024], P(None, 'tp'), may hold values from -0.375 to 0.375
- rec_value: bfloat16 [2048, 1024], P(None, 'tp'), may hold values from -0.125 to 0.125
- gate_gap: float32 [2, 1024], P(None, 'tp'), may hold values from 0.00012207031 to 0.12
- extra_decay: float32 [2, 8192, 8], P(None, 'sp', 'tp'), may hold values from -0.7 to 0
- init_state: float32 [2, 8, 128, 128], P(None, 'tp'), may hold values from -0.5 to 0.5
- rec_gain: float32 [128], replicated, may hold values from 0.1 to 1.9
- out_attn: bfloat16 [1024, 2048], P('tp'), may hold values from -0.125 to 0.125
- out_rec: bfloat16 [1024, 2048], P('tp'), may hold values from -0.125 to 0.125
Outputs:
- mixed: bfloat16 [8192, 2048], P(('sp', 'tp'))
The draws below stay inside these ranges and needn't reach their ends.
Inputs may be any that keep to these rules, and one draw needn't show every extreme that they name: `da_query`: entries lie within -240 / sqrt(2048) and 240 / sqrt(2048).
All inputs are finite; a program needn't handle non-finite values.
Results may differ from the reference program's by a relative error of at most 0.014.
The reference program's roundings to bfloat16 on the way count: a program that leaves them out, or rounds other values in their place, can miss the bound.
Values may be sent and summed in bfloat16 or wider, within the bound.
No kernel may reach another device: no remote copies, remote signals or barrier semaphores. Data moves between devices by JAX's collectives and lax.ppermute only.
A program may use at most 128 MiB of HBM per device.

```python
import math
import jax
import jax.numpy as jnp
from jax import lax

D = 2048
DA_HEADS = 8
QK_DIM = 64
DA_VAL = 128
RECURRENT_HEADS = 8
HG_KEY = 128
HG_VAL = 128
SPAN = 64
TOK_DEV = 128
TOKEN_COUNT = 8192


def draw_da_query(key, part):
    spread = 1.8
    base = jnp.clip(jax.random.normal(key, (D, DA_HEADS * 2 * QK_DIM), jnp.float32), -6.0, 6.0)
    return (base * (spread / math.sqrt(D))).astype(jnp.bfloat16)


def draw_gate_gap(key, part):
    head_key, slow_key, fast_key = jax.random.split(jax.random.fold_in(key, 11), 3)
    chance = 0.5
    slow_heads = jax.random.uniform(head_key, (2, RECURRENT_HEADS, 1), jnp.float32) < chance
    slow_gap = jax.random.uniform(slow_key, (2, RECURRENT_HEADS, HG_KEY), jnp.float32, 1.0, 3.0) / TOKEN_COUNT
    fast_gap = jnp.exp(jax.random.uniform(fast_key, (2, RECURRENT_HEADS, HG_KEY), jnp.float32, math.log(0.04), math.log(0.12)))
    return jnp.where(slow_heads, slow_gap, fast_gap).reshape(2, RECURRENT_HEADS * HG_KEY).astype(jnp.float32)


def draw_extra_decay(key, part):
    rate_key, key_position, depth_key = jax.random.split(jax.random.fold_in(key, 23), 3)
    half_rows = max(TOK_DEV // 2, 1)
    block_count = TOKEN_COUNT // half_rows
    rates = jnp.exp(jax.random.uniform(rate_key, (2, block_count, 1, RECURRENT_HEADS), jnp.float32, math.log(0.3), math.log(3.0)))
    steady_decay = jnp.broadcast_to(-rates / TOKEN_COUNT, (2, block_count, half_rows, RECURRENT_HEADS)).reshape(2, TOKEN_COUNT, RECURRENT_HEADS)
    sudden_inputs = jax.random.uniform(key_position, (2, TOKEN_COUNT, RECURRENT_HEADS), jnp.float32) < 4.0 / TOKEN_COUNT
    decay_drops = jnp.log(jax.random.uniform(depth_key, (2, TOKEN_COUNT, RECURRENT_HEADS), jnp.float32, 0.5, 0.8))
    return jnp.where(sudden_inputs, decay_drops, steady_decay).astype(jnp.float32)


def block_scale(rng, dims, pieces, smallest, largest):
    loudness, own = 1.0, jax.random.fold_in(rng, 6)
    for position, blocks in pieces:
        draws = jnp.exp(jax.random.uniform(jax.random.fold_in(own, position), (blocks,), jnp.float32, smallest / len(pieces), largest / len(pieces)))
        loudness = loudness * jnp.repeat(draws, dims[position] // blocks).reshape([-1 if axis == position else 1 for axis in range(len(dims))])
    return loudness


def noise(key, extent, deviation, limit, pieces=(), kind=jnp.bfloat16):
    values = jax.random.normal(key, extent, jnp.float32) * deviation
    if len(pieces) > 0:
        values = block_scale(key, extent, pieces, -0.22, 0.18) * values
    return jnp.clip(values, min=-limit, max=limit).astype(kind)


def setup_inputs(seed: int = 0) -> dict:
    key_of = jax.random.split(jax.random.key(seed), 18)
    tokens = noise(key_of[0], (TOKEN_COUNT, D), 1.0, 6.0, ((0, 64), (1, 4)))
    norm_gain = jnp.clip(1.0 + 0.18 * jax.random.normal(key_of[1], (D,), jnp.float32), 0.1, 1.9)
    da_query = draw_da_query(jax.random.fold_in(key_of[17], 71), 0)
    da_key = noise(key_of[3], (D, DA_HEADS * 2 * QK_DIM), D ** -0.5, 0.125, ((1, 4),))
    da_value = noise(key_of[4], (D, DA_HEADS * DA_VAL), D ** -0.5, 0.125, ((1, 4),))
    mix_lambda = jnp.clip(0.3 + 0.5 * jax.random.uniform(key_of[5], (DA_HEADS,), jnp.float32) ** block_scale(key_of[5], (DA_HEADS,), ((0, 4),), -0.2, 0.2), 0.3, 0.8)
    attn_gain = jnp.clip(1.0 + 0.18 * jax.random.normal(key_of[6], (DA_VAL,), jnp.float32), 0.1, 1.9)
    rec_query = noise(key_of[7], (D, RECURRENT_HEADS * HG_KEY), D ** -0.5, 0.125, ((1, 4),))
    rec_forget_fwd = noise(key_of[8], (D, RECURRENT_HEADS * HG_KEY), (D // 8) ** -0.5, 0.375, ((1, 4),))
    rec_forget_bwd = noise(key_of[9], (D, RECURRENT_HEADS * HG_KEY), (D // 8) ** -0.5, 0.375, ((1, 4),))
    rec_value = noise(key_of[10], (D, RECURRENT_HEADS * HG_VAL), D ** -0.5, 0.125, ((1, 4),))
    gate_gap = draw_gate_gap(jax.random.fold_in(key_of[17], 71), 0)
    extra_decay = draw_extra_decay(jax.random.fold_in(key_of[17], 71), 0)
    init_state = noise(key_of[13], (2, RECURRENT_HEADS, HG_KEY, HG_VAL), (3.0 * TOKEN_COUNT ** -0.5), 0.5, ((1, 4),), jnp.float32)
    rec_gain = jnp.clip(1.0 + 0.18 * jax.random.normal(key_of[14], (HG_VAL,), jnp.float32), 0.1, 1.9)
    out_attn = noise(key_of[15], (DA_HEADS * DA_VAL, D), (DA_HEADS * DA_VAL + RECURRENT_HEADS * HG_VAL) ** -0.5, 0.125, ((0, 4),))
    out_rec = noise(key_of[16], (RECURRENT_HEADS * HG_VAL, D), (DA_HEADS * DA_VAL + RECURRENT_HEADS * HG_VAL) ** -0.5, 0.125, ((0, 4),))
    return {"tokens": tokens, "norm_gain": norm_gain, "da_query": da_query, "da_key": da_key, "da_value": da_value, "mix_lambda": mix_lambda, "attn_gain": attn_gain, "rec_query": rec_query, "rec_forget_fwd": rec_forget_fwd, "rec_forget_bwd": rec_forget_bwd, "rec_value": rec_value, "gate_gap": gate_gap, "extra_decay": extra_decay, "init_state": init_state, "rec_gain": rec_gain, "out_attn": out_attn, "out_rec": out_rec}


EPSILON = 1e-06
EXACT_PRECISION = lax.Precision.HIGHEST

def block_scan(query, key_in, values, log_decay, initial):
    length = query.shape[0]
    count = length // SPAN

    def split(array):
        return array.reshape((count, SPAN) + array.shape[1:])
    lower = jnp.tril(jnp.ones((SPAN, SPAN), jnp.float32))

    def one_step(carried_state, inputs):
        query_tile, key_tile, value_tile, g_block = inputs
        cumulative_decay = jnp.cumsum(g_block, axis=0)
        relative = cumulative_decay[:, None] - cumulative_decay[None, :]
        relative = jnp.where(lower[:, :, None, None] > 0, relative, -jnp.inf)
        score_matrix = jnp.einsum('ihk,ijhk,jhk->hij', query_tile, jnp.exp(relative), key_tile, precision=EXACT_PRECISION)
        output_rows = jnp.einsum('ujg,jga->uja', query_tile * jnp.exp(cumulative_decay), carried_state, precision=EXACT_PRECISION) + jnp.einsum('ots,sok->tok', score_matrix, value_tile, precision=EXACT_PRECISION)
        ending_state = cumulative_decay[-1]
        carried_state = jnp.exp(ending_state)[..., None] * carried_state + jnp.einsum('zds,zdx->dsx', key_tile * jnp.exp(ending_state[None] - cumulative_decay), value_tile, precision=EXACT_PRECISION)
        return (carried_state, output_rows)
    carried_state, output_rows = lax.scan(one_step, initial, (split(query), split(key_in), split(values), split(log_decay)))
    return (output_rows.reshape((length,) + output_rows.shape[2:]), carried_state)

def reference(tokens, norm_gain, da_query, da_key, da_value, mix_lambda, attn_gain, rec_query, rec_forget_fwd, rec_forget_bwd, rec_value, gate_gap, extra_decay, init_state, rec_gain, out_attn, out_rec):
    values = tokens.astype(jnp.float32)
    scaled = (values * norm_gain).astype(jnp.bfloat16)
    inv_rms = lax.rsqrt(lax.optimization_barrier(jnp.mean(values * values, axis=1, keepdims=True)) + EPSILON)

    def project(weight):
        return (jnp.dot(scaled, weight, preferred_element_type=jnp.float32) * inv_rms).astype(jnp.bfloat16)
    query_att = project(da_query).reshape(TOKEN_COUNT, DA_HEADS, 2, QK_DIM)
    key_att = project(da_key).reshape(TOKEN_COUNT, DA_HEADS, 2, QK_DIM).astype(jnp.float32)
    value_att = project(da_value).reshape(TOKEN_COUNT, DA_HEADS, DA_VAL).astype(jnp.float32)
    query_rows = math.gcd(TOKEN_COUNT, 256)
    query_blocks = query_att.reshape(TOKEN_COUNT // query_rows, query_rows, DA_HEADS, 2, QK_DIM)

    def attend(query_block):
        score_matrix = jnp.einsum('qhmd,khmd->hmqk', query_block.astype(jnp.float32), key_att) * QK_DIM ** (-0.5)
        maxima = lax.optimization_barrier(jnp.max(score_matrix, axis=3, keepdims=True))
        unnorm = jnp.exp(score_matrix - maxima)
        denoms = lax.optimization_barrier(jnp.sum(unnorm, axis=3))
        rounded = lax.optimization_barrier(unnorm.astype(jnp.bfloat16)).astype(jnp.float32)
        numerator = jnp.einsum('hmqk,khv->hmqv', rounded, value_att)
        ratio = numerator / denoms[..., None]
        diff = ratio[:, 0] - mix_lambda[:, None, None] * ratio[:, 1]
        normed = diff * lax.rsqrt(lax.optimization_barrier(jnp.mean(diff * diff, axis=-1, keepdims=True)) + EPSILON) * attn_gain
        return jnp.transpose(normed, (1, 0, 2)).astype(jnp.bfloat16)
    attn_out = lax.map(attend, query_blocks).reshape(TOKEN_COUNT, DA_HEADS * DA_VAL)

    def heads(array, width):
        return array.astype(jnp.float32).reshape(TOKEN_COUNT, RECURRENT_HEADS, width)
    rec_q = jax.nn.silu(heads(project(rec_query), HG_KEY)) * HG_KEY ** (-0.5)
    values_rec = heads(project(rec_value), HG_VAL)
    forgets = (project(rec_forget_fwd), project(rec_forget_bwd))
    outputs = []
    for direction in range(2):
        gap = gate_gap[direction].reshape(RECURRENT_HEADS, HG_KEY)
        key_in = gap * jax.nn.sigmoid(-heads(forgets[direction], HG_KEY))
        log_decay = jnp.log1p(-key_in) + extra_decay[direction][:, :, None]
        if direction == 0:
            result, unused = block_scan(rec_q, key_in, values_rec, log_decay, init_state[0])
        else:
            result, unused = block_scan(rec_q[::-1], key_in[::-1], values_rec[::-1], log_decay[::-1], init_state[1])
            result = result[::-1]
        outputs.append(result)
    rec_sum = outputs[0] + outputs[1]
    rec_normed = rec_sum * lax.rsqrt(lax.optimization_barrier(jnp.mean(rec_sum * rec_sum, axis=-1, keepdims=True)) + EPSILON) * rec_gain
    rec_out = rec_normed.reshape(TOKEN_COUNT, RECURRENT_HEADS * HG_VAL).astype(jnp.bfloat16)
    mixed = jnp.dot(attn_out, out_attn, preferred_element_type=jnp.float32) + jnp.dot(rec_out, out_rec, preferred_element_type=jnp.float32)
    return mixed.astype(jnp.bfloat16)
```

```python
import functools

import jax
import jax.numpy as jnp
from jax import lax
from jax.experimental import pallas as pl
from jax.experimental.pallas import tpu as pltpu
from jax.sharding import Mesh
from jax.sharding import PartitionSpec as P

D = 2048
QK_DIM = 64
HG_KEY = 128
EPSILON = 1e-06
LOG2E = 1.4426950408889634
Z, X, C, Y = ("z", "x", "c", "y")
SP = (Z, X, C)
F32 = jnp.float32
BF16 = jnp.bfloat16


VMEM = pl.BlockSpec(memory_space=pltpu.VMEM)
SMEM = pl.BlockSpec(memory_space=pltpu.SMEM)


def call(body, out, ins, scratch=(), specs=None, flops=0):
    one = isinstance(out, tuple)
    outs = [out] if one else list(out)
    shapes = [jax.ShapeDtypeStruct(s, t) for s, t in outs]
    specs = specs or [VMEM] * len(ins)
    done = pl.pallas_call(
        body,
        out_shape=shapes,
        in_specs=specs,
        out_specs=[VMEM] * len(shapes),
        scratch_shapes=list(scratch),
        cost_estimate=pl.CostEstimate(flops=flops, transcendentals=0, bytes_accessed=0),
        compiler_params=pltpu.CompilerParams(vmem_limit_bytes=48 << 20),
    )(*ins)
    return done[0] if one else done


def dot(a, b):
    return lax.dot_general(a, b, (((1,), (0,)), ((), ())), preferred_element_type=F32)


def dot_nt(a, b):
    return lax.dot_general(a, b, (((1,), (1,)), ((), ())), preferred_element_type=F32)


def dot_tn(a, b):
    return lax.dot_general(a, b, (((0,), (0,)), ((), ())), preferred_element_type=F32)


def shifted(value, axis, by):
    peers = lax.axis_size(axis)
    return lax.ppermute(value, axis, [(i, (i + by) % peers) for i in range(peers)])


def project_attention(tok, gain, wq, wk, wv, q_out, kv_out, scaled_out, inv_out):
    blocks = tok.shape[0]
    width = tok.shape[2]
    squares = None
    for b in range(blocks):
        values = tok[b].astype(F32)
        part = jnp.sum(values * values, axis=1, keepdims=True)
        squares = part if squares is None else squares + part
        at = slice(b * width, (b + 1) * width)
        scaled_out[:, at] = (values * gain[:, at]).astype(BF16)
    inv = lax.rsqrt(squares / (blocks * width) + EPSILON)
    inv_out[...] = jnp.broadcast_to(inv, inv_out.shape)
    scaled = scaled_out[...]
    wide = q_out.shape[1]
    kv_out[:, :wide] = (dot(scaled, wk[...]) * inv).astype(BF16)
    kv_out[:, wide:] = (dot(scaled, wv[...]) * inv).astype(BF16)
    q_out[...] = (dot(scaled, wq[...]) * inv).astype(BF16)


def triangle_sum(ones, value):
    high = value.astype(BF16)
    rest = value - high.astype(F32)
    middle = rest.astype(BF16)
    low = (rest - middle.astype(F32)).astype(BF16)
    return dot(ones, high) + dot(ones, middle) + dot(ones, low)


def recurrence_local(scaled, inv_ref, wq, wf, wb, wv, gap, extra, out, qf_out, qb_out, send):
    x = scaled[...]
    inv = inv_ref[:, :1]
    rows = x.shape[0]
    width = wq.shape[1]
    heads = width // HG_KEY

    def project(w):
        return (dot(x, w[...]) * inv).astype(BF16)

    rv = project(wv)
    rq = project(wq).astype(F32)
    rec_q = rq / (1.0 + jnp.exp(-rq)) * HG_KEY**-0.5
    row = lax.broadcasted_iota(jnp.int32, (rows, rows), 0)
    col = lax.broadcasted_iota(jnp.int32, (rows, rows), 1)
    scores = [None] * heads
    for d, w in enumerate((wf, wb)):
        forget = project(w).astype(F32)
        key = gap[d : d + 1, :] / (1.0 + jnp.exp(forget))
        keep = (row >= col) if d == 0 else (row <= col)
        more = jnp.concatenate(
            [
                jnp.broadcast_to(extra[d * rows : (d + 1) * rows, h : h + 1], (rows, HG_KEY))
                for h in range(heads)
            ],
            axis=1,
        )
        decay = jnp.log1p(-key) + more
        total = triangle_sum(keep.astype(BF16), decay)
        last = rows - 1 if d == 0 else 0
        end = total[last : last + 1, :]
        middle = total[rows // 2 : rows // 2 + 1, :]
        near_q = (rec_q * jnp.exp(total - middle)).astype(BF16)
        near_k = (key * jnp.exp(middle - total)).astype(BF16)
        (qf_out if d == 0 else qb_out)[...] = (rec_q * jnp.exp(total)).astype(BF16)
        far_k = (key * jnp.exp(end - total)).astype(BF16)
        high = end.astype(BF16).astype(F32)
        low = end - high
        pieces = HG_KEY // 8
        for h in range(heads):
            at = slice(h * HG_KEY, (h + 1) * HG_KEY)
            s = jnp.where(keep, dot_nt(near_q[:, at], near_k[:, at]), 0.0)
            scores[h] = s if scores[h] is None else scores[h] + s
            state = dot_tn(rv[:, at], far_k[:, at]).reshape(pieces, 8, HG_KEY)
            sub = lax.broadcasted_iota(jnp.int32, (8, HG_KEY), 0)
            tail = jnp.where(sub == 0, high[:, at], jnp.where(sub == 1, low[:, at], 0.0))
            tail = jnp.broadcast_to(tail[None], (pieces, 8, HG_KEY))
            first = (d * heads + h) * pieces
            send[first : first + pieces] = jnp.concatenate([state, tail], axis=1).astype(BF16)
    for h in range(heads):
        at = slice(h * HG_KEY, (h + 1) * HG_KEY)
        out[:, at] = dot(scores[h].astype(BF16), rv[:, at])


def entering_states(place, got, init, send, turned):
    me = place[0]
    peers = got.shape[0]
    pieces = HG_KEY // 8
    which = me // pieces
    turned[...] = init[which].T
    state = turned[pl.ds((me % pieces) * 8, 8), :]
    backward = me >= peers // 2
    for t in range(peers):
        at = jnp.where(backward, peers - 1 - t, t)
        send[at] = state.astype(BF16)
        piece = got[at].astype(F32)
        decay = piece[8:9, :] + piece[9:10, :]
        state = jnp.exp(decay) * state + piece[:8, :]


def absorb(place, q0, q1, q2, q3, kv, most_in, sums_in, most_out, sums_out, final):
    heads = q0.shape[1] // 128
    keys = kv.shape[0] * kv.shape[1]
    rows = q0.shape[0]
    wide = heads * 128
    lane = lax.broadcasted_iota(jnp.int32, (rows, 128), 1)
    diagonal = lax.broadcasted_iota(jnp.int32, (rows, 128), 0) == lane
    scale = QK_DIM**-0.5 * LOG2E
    for h in range(heads):
        at = slice(h * 128, (h + 1) * 128)
        key = kv[:, :, at].reshape(keys, 128)
        val = kv[:, :, wide + h * 128 : wide + (h + 1) * 128].reshape(keys, 128)
        val = jnp.concatenate([val, jnp.ones((keys, 128), BF16)], axis=1)
        for s, q in enumerate((q0, q1, q2, q3)):
            n = h * 4 + s
            query = q[:, at]
            none = jnp.zeros_like(query)
            both = jnp.concatenate(
                [jnp.where(lane < QK_DIM, query, none), jnp.where(lane < QK_DIM, none, query)],
                axis=0,
            )
            score = dot_nt(both, key)
            most = jnp.max(score, axis=1, keepdims=True)
            if most_in is not None:
                old = most_in[n][:, :1]
                most = jnp.maximum(most, old)
            weight = jnp.exp2((score - most) * scale).astype(BF16)
            sums = dot(weight, val)
            if most_in is not None:
                sums = sums + jnp.exp2((old - most) * scale) * sums_in[n]
            if final is None:
                most_out[n] = jnp.broadcast_to(most, (2 * rows, 128))
                sums_out[n] = sums
                continue
            target = (place[0] + 4 - s) % 4
            norm = sums[:, 128:]
            final[target, h * 2 * rows : (h + 1) * 2 * rows, :] = (sums[:, :128] / norm).astype(
                BF16
            )
            level = most * scale + jnp.log2(norm)
            lines = [
                jnp.sum(jnp.where(diagonal, level[m * rows : (m + 1) * rows], 0.0), 0, keepdims=True)
                for m in range(2)
            ]
            line = jnp.concatenate(lines, axis=0)
            high = line.astype(BF16)
            rest = line - high.astype(F32)
            middle = rest.astype(BF16)
            low = (rest - middle.astype(F32)).astype(BF16)
            fill = jnp.zeros((10, 128), F32)
            tail = jnp.concatenate(
                [high.astype(F32), middle.astype(F32), low.astype(F32), fill], axis=0
            )
            base = heads * 2 * rows + h * 16
            final[target, base : base + 16, :] = tail.astype(BF16)


def absorb_first(place, q0, q1, q2, q3, kv, most_out, sums_out):
    absorb(place, q0, q1, q2, q3, kv, None, None, most_out, sums_out, None)


def absorb_last(place, q0, q1, q2, q3, kv, most_in, sums_in, final):
    absorb(place, q0, q1, q2, q3, kv, most_in, sums_in, None, None, final)


def finish(parts, lam, gain_a, out_l, qf, qb, states, gain_r, wa, wr, mixed):
    peers = parts.shape[0]
    rows = out_l.shape[0]
    heads = out_l.shape[1] // 128
    row = lax.broadcasted_iota(jnp.int32, (rows, 128), 0)
    diagonal = row == lax.broadcasted_iota(jnp.int32, (rows, 128), 1)
    attn = []
    rec = []
    for h in range(heads):
        ratio = []
        for m in range(2):
            levels = []
            for p in range(peers):
                tail = parts[p, heads * 2 * rows + h * 16 : heads * 2 * rows + h * 16 + 16, :]
                tail = tail.astype(F32)
                line = tail[m : m + 1] + tail[m + 2 : m + 3] + tail[m + 4 : m + 5]
                levels.append(jnp.sum(jnp.where(diagonal, line, 0.0), axis=1, keepdims=True))
            top = functools.reduce(jnp.maximum, levels)
            shares = [jnp.exp2(v - top) for v in levels]
            norm = functools.reduce(jnp.add, shares)
            at = slice((h * 2 + m) * rows, (h * 2 + m + 1) * rows)
            both = functools.reduce(
                jnp.add, [w * parts[p, at, :].astype(F32) for p, w in enumerate(shares)]
            )
            ratio.append(both / norm)
        diff = ratio[0] - lam[h] * ratio[1]
        mean = jnp.mean(diff * diff, axis=1, keepdims=True)
        attn.append((diff * lax.rsqrt(mean + EPSILON) * gain_a[...]).astype(BF16))
        at = slice(h * 128, (h + 1) * 128)
        total = out_l[:, at]
        for d, q in enumerate((qf, qb)):
            first = (d * heads + h) * 16
            state = states[first : first + 16].astype(F32).reshape(HG_KEY, HG_KEY).astype(BF16)
            total = total + dot_nt(q[:, at], state)
        mean = jnp.mean(total * total, axis=1, keepdims=True)
        rec.append((total * lax.rsqrt(mean + EPSILON) * gain_r[...]).astype(BF16))
    attn = jnp.concatenate(attn, axis=1)
    rec = jnp.concatenate(rec, axis=1)
    result = dot(attn, wa[...]) + dot(rec, wr[...])
    pieces = mixed.shape[0]
    mixed[...] = result.astype(BF16).reshape(pieces, rows // pieces, result.shape[1])


def add_up(parts, out):
    total = functools.reduce(jnp.add, [parts[p].astype(F32) for p in range(parts.shape[0])])
    out[...] = total.astype(BF16)


def local(
    tokens,
    norm_gain,
    da_query,
    da_key,
    da_value,
    mix_lambda,
    attn_gain,
    rec_query,
    rec_forget_fwd,
    rec_forget_bwd,
    rec_value,
    gate_gap,
    extra_decay,
    init_state,
    rec_gain,
    out_attn,
    out_rec,
):
    rows, width = tokens.shape
    tp = lax.axis_size(Y)
    wide = da_query.shape[1]
    x_here = lax.axis_index(X)[None]
    sp_here = lax.axis_index(SP)[None]

    def spread(value, axis):
        copies = jnp.broadcast_to(value, (lax.axis_size(axis), *value.shape))
        return lax.all_to_all(copies, axis, 0, 0, tiled=True)

    tok = spread(tokens, Y)
    query, kv, scaled, inv = call(
        project_attention,
        [((rows, wide), BF16), ((rows, 2 * wide), BF16), ((rows, D), BF16), ((rows, 128), F32)],
        [tok, norm_gain[None], da_query, da_key, da_value],
        flops=2 * rows * D * 3 * wide,
    )
    kv_z = spread(kv, Z)
    queries = [query] + [shifted(query, X, s) for s in (1, 3, 2)]
    queries = [queries[0], queries[1], queries[3], queries[2]]

    out_l, qf, qb, send = call(
        recurrence_local,
        [
            ((rows, wide), F32),
            ((rows, wide), BF16),
            ((rows, wide), BF16),
            ((64, 16, 128), BF16),
        ],
        [
            scaled,
            inv,
            rec_query,
            rec_forget_fwd,
            rec_forget_bwd,
            rec_value,
            gate_gap,
            extra_decay.reshape(2 * rows, -1),
        ],
        flops=2 * rows * D * 4 * wide * 2,
    )
    send, kv_z = lax.optimization_barrier((send, kv_z))
    kv_c = shifted(kv_z, C, 1)
    got = lax.all_to_all(send, SP, 0, 0, tiled=True)
    back = call(
        entering_states,
        ((64, 8, 128), BF16),
        [sp_here, got, init_state.reshape(-1, HG_KEY, HG_KEY)],
        scratch=[pltpu.VMEM((HG_KEY, HG_KEY), F32)],
        specs=[SMEM, VMEM, VMEM],
    )
    states = lax.all_to_all(back, SP, 0, 0, tiled=True)

    groups = 4 * (wide // 128)
    flops = 2 * groups * 2 * rows * 8 * rows * 256 * 2
    most, sums = call(
        absorb_first,
        [((groups, 2 * rows, 128), F32), ((groups, 2 * rows, 256), F32)],
        [x_here, *queries, kv_z],
        specs=[SMEM] + [VMEM] * 5,
        flops=flops,
    )
    parts = call(
        absorb_last,
        ((4, 2 * wide + 16 * (wide // 128), 128), BF16),
        [x_here, *queries, kv_c, most, sums],
        specs=[SMEM] + [VMEM] * 7,
        flops=flops,
    )
    parts = lax.all_to_all(parts, X, 0, 0, tiled=True)
    mixed = call(
        finish,
        ((tp, rows // tp, D), BF16),
        [
            parts,
            mix_lambda,
            attn_gain[None],
            out_l,
            qf,
            qb,
            states,
            rec_gain[None],
            out_attn,
            out_rec,
        ],
        specs=[VMEM, SMEM] + [VMEM] * 8,
        flops=2 * rows * D * 2 * wide,
    )
    mixed = lax.all_to_all(mixed, Y, 0, 0, tiled=True)
    return call(add_up, ((rows // tp, D), BF16), [mixed])


def solution(mesh):
    torus = Mesh(mesh.devices.reshape(8, 4, 2, mesh.shape["tp"]), (Z, X, C, Y))
    return jax.shard_map(
        local,
        mesh=torus,
        in_specs=(
            P(SP, Y),
            P(),
            P(None, Y),
            P(None, Y),
            P(None, Y),
            P(Y),
            P(),
            P(None, Y),
            P(None, Y),
            P(None, Y),
            P(None, Y),
            P(None, Y),
            P(None, SP, Y),
            P(None, Y, None, None),
            P(),
            P(Y, None),
            P(Y, None),
        ),
        out_specs=P((*SP, Y), None),
        check_vma=False,
    )
```

```python
import functools

import jax
import jax.numpy as jnp
from jax import lax
from jax.experimental import pallas as pl
from jax.experimental.pallas import tpu as pltpu
from jax.sharding import Mesh
from jax.sharding import PartitionSpec as P

D = 2048
QK_DIM = 64
HG_KEY = 128
EPSILON = 1e-06
LOG2E = 1.4426950408889634
Z, X, C, Y = ("z", "x", "c", "y")
SP = (Z, X, C)
F32 = jnp.float32
BF16 = jnp.bfloat16


VMEM = pl.BlockSpec(memory_space=pltpu.VMEM)
SMEM = pl.BlockSpec(memory_space=pltpu.SMEM)
HBM = pl.BlockSpec(memory_space=pltpu.HBM)


def call(body, out, ins, scratch=(), specs=None, flops=0, mib=4):
    one = isinstance(out, tuple)
    outs = [out] if one else list(out)
    shapes = [jax.ShapeDtypeStruct(s, t) for s, t in outs]
    specs = specs or [VMEM] * len(ins)
    done = pl.pallas_call(
        body,
        out_shape=shapes,
        in_specs=specs,
        out_specs=[VMEM] * len(shapes),
        scratch_shapes=list(scratch),
        cost_estimate=pl.CostEstimate(flops=flops, transcendentals=0, bytes_accessed=0),
        compiler_params=pltpu.CompilerParams(vmem_limit_bytes=mib << 20),
    )(*ins)
    return done[0] if one else done


def dot(a, b):
    return lax.dot_general(a, b, (((1,), (0,)), ((), ())), preferred_element_type=F32)


def dot_nt(a, b):
    return lax.dot_general(a, b, (((1,), (1,)), ((), ())), preferred_element_type=F32)


def dot_tn(a, b):
    return lax.dot_general(a, b, (((0,), (0,)), ((), ())), preferred_element_type=F32)


def shifted(value, axis, by):
    peers = lax.axis_size(axis)
    return lax.ppermute(value, axis, [(i, (i + by) % peers) for i in range(peers)])


def project(tags, t0, t1, t2, t3, gain, *refs):
    weights = refs[:7]
    mine, theirs, held, sems = refs[7:]
    copies = [
        pltpu.make_async_copy(w, held.at[n], sems.at[n]) for n, w in enumerate(weights)
    ]
    for copy in copies:
        copy.start()
    core = tags[0]
    here = tags[1]
    rows, width = t0.shape
    squares = None
    pieces = []
    starts = []
    for s, tok in enumerate((t0, t1, t2, t3)):
        start = ((here + 4 - s) % 4) * width
        values = tok[...].astype(F32)
        part = jnp.sum(values * values, axis=1, keepdims=True)
        squares = part if squares is None else squares + part
        scale = gain[(here + 4 - s) % 4]
        pieces.append((values * scale).astype(BF16))
        starts.append(pl.multiple_of(start, width))
    inv = lax.rsqrt(squares / (4 * width) + EPSILON)
    for n, copy in enumerate(copies):
        copy.wait()
        total = None
        for piece, start in zip(pieces, starts):
            part = dot(piece, held[n, pl.ds(start, width), :])
            total = part if total is None else total + part
        total = (total * inv).astype(BF16)
        at = slice(n * 128, (n + 1) * 128)
        first = total[:, :128]
        second = total[:, 128:]
        mine[:, at] = jnp.where(core == 0, first, second)
        theirs[:, at] = jnp.where(core == 0, second, first)


def join(tags, mine, got, kv, query):
    core = tags[0]
    rows = mine.shape[0]
    for ref, place in ((mine, core), (got, 1 - core)):
        at = pl.ds(pl.multiple_of(place * rows, rows), rows)
        kv[at, :] = ref[:, :256]
        query[at, :] = ref[:, 256:384]


def triangle_sum(ones, value):
    high = value.astype(BF16)
    rest = value - high.astype(F32)
    middle = rest.astype(BF16)
    low = (rest - middle.astype(F32)).astype(BF16)
    return dot(ones, high) + dot(ones, middle) + dot(ones, low)


def recurrence_local(tags, mine, got, gap, extra, far, kept, send):
    core = tags[0]
    rows = mine.shape[0]
    row = lax.broadcasted_iota(jnp.int32, (rows, rows), 0)
    col = lax.broadcasted_iota(jnp.int32, (rows, rows), 1)
    sub = lax.broadcasted_iota(jnp.int32, (8, HG_KEY), 0)
    a = mine[:, 384:]
    b = got[:, 384:]
    blocks = (jnp.where(core == 0, a, b), jnp.where(core == 0, b, a))
    values = [x[:, :128] for x in blocks]
    rec_q = []
    for x in blocks:
        rq = x[:, 128:256].astype(F32)
        rec_q.append(rq / (1.0 + jnp.exp(-rq)) * HG_KEY**-0.5)
    out = [None, None]
    pieces = HG_KEY // 8
    for d in range(2):
        keep = (row >= col) if d == 0 else (row <= col)
        ones = keep.astype(BF16)
        pair = gap[d : d + 1, :]
        share = jnp.where(core == 0, pair[:, :128], pair[:, 128:])
        order = (0, 1) if d == 0 else (1, 0)
        state = None
        before = None
        for n in order:
            forget = blocks[n][:, (2 + d) * 128 : (3 + d) * 128].astype(F32)
            key = share / (1.0 + jnp.exp(forget))
            mine_line = extra[d * 2 : d * 2 + 1, :]
            got_line = far[d * 2 : d * 2 + 1, :]
            line0 = jnp.where(core == n, mine_line, got_line)
            mine_line = extra[d * 2 + 1 : d * 2 + 2, :]
            got_line = far[d * 2 + 1 : d * 2 + 2, :]
            line1 = jnp.where(core == n, mine_line, got_line)
            line = jnp.where(core == 0, line0, line1)
            more = jnp.sum(jnp.where(keep, line, 0.0), axis=1, keepdims=True)
            total = triangle_sum(ones, jnp.log1p(-key)) + more
            last = rows - 1 if d == 0 else 0
            end = total[last : last + 1, :]
            middle = total[rows // 2 : rows // 2 + 1, :]
            near_q = (rec_q[n] * jnp.exp(total - middle)).astype(BF16)
            near_k = (key * jnp.exp(middle - total)).astype(BF16)
            score = jnp.where(keep, dot_nt(near_q, near_k), 0.0).astype(BF16)
            result = dot(score, values[n])
            far_k = (key * jnp.exp(end - total)).astype(BF16)
            piece = dot_tn(values[n], far_k)
            if state is None:
                state = piece
                before = end
                reach = total
            else:
                near = (rec_q[n] * jnp.exp(total)).astype(BF16)
                result = result + dot_nt(near, state.astype(BF16))
                state = jnp.exp(end) * state + piece
                reach = total + before
                before = before + end
            kept[n * rows : (n + 1) * rows, (1 + d) * 128 : (2 + d) * 128] = rec_q[n] * jnp.exp(
                reach
            )
            out[n] = result if out[n] is None else out[n] + result
        high = before.astype(BF16).astype(F32)
        low = before - high
        tail = jnp.where(sub == 0, high, jnp.where(sub == 1, low, 0.0))
        tail = jnp.broadcast_to(tail[None], (pieces, 8, HG_KEY))
        both = jnp.concatenate([state.reshape(pieces, 8, HG_KEY), tail], axis=1)
        send[d * pieces : (d + 1) * pieces] = both.astype(BF16)
    for n in range(2):
        kept[n * rows : (n + 1) * rows, :128] = out[n]


def entering_states(tags, got, init, send, turned):
    me = tags[3]
    peers = got.shape[0]
    pieces = HG_KEY // 8
    which = (me // pieces) * 2 + tags[0]
    turned[...] = init[which].T
    state = turned[pl.ds(pl.multiple_of((me % pieces) * 8, 8), 8), :]
    backward = me >= peers // 2
    for t in range(peers):
        at = jnp.where(backward, peers - 1 - t, t)
        send[at] = state.astype(BF16)
        piece = got[at].astype(F32)
        decay = piece[8:9, :] + piece[9:10, :]
        state = jnp.exp(decay) * state + piece[:8, :]


def absorb(tags, queries, pieces, most_in, sums_in, most_out, sums_out, final):
    rows = queries[0].shape[0]
    lane = lax.broadcasted_iota(jnp.int32, (rows, 128), 1)
    row = lax.broadcasted_iota(jnp.int32, (128, 128), 0)
    diagonal = row == lax.broadcasted_iota(jnp.int32, (128, 128), 1)
    scale = QK_DIM**-0.5 * LOG2E
    key = jnp.concatenate([p[:, :128] for p in pieces], axis=0)
    val = jnp.concatenate([p[:, 128:] for p in pieces], axis=0)
    val = jnp.concatenate([val, jnp.ones(val.shape, BF16)], axis=1)
    for s, q in enumerate(queries):
        query = q[...]
        none = jnp.zeros_like(query)
        both = jnp.concatenate(
            [jnp.where(lane < QK_DIM, query, none), jnp.where(lane < QK_DIM, none, query)],
            axis=0,
        )
        score = dot_nt(both, key)
        most = jnp.max(score, axis=1, keepdims=True)
        if most_in is not None:
            old = most_in[s][:, :1]
            most = jnp.maximum(most, old)
        weight = jnp.exp2((score - most) * scale).astype(BF16)
        sums = dot(weight, val)
        if most_in is not None:
            sums = sums + jnp.exp2((old - most) * scale) * sums_in[s]
        if final is None:
            most_out[s] = jnp.broadcast_to(most, (2 * rows, 128))
            sums_out[s] = sums
            continue
        target = (tags[2] + 4 - s) % 4
        norm = sums[:, 128:]
        final[target, : 2 * rows, :] = (sums[:, :128] / norm).astype(BF16)
        level = most * scale + jnp.log2(norm)
        lines = [
            jnp.sum(jnp.where(diagonal, level[m * 128 : (m + 1) * 128], 0.0), 0, keepdims=True)
            for m in range(2 * rows // 128)
        ]
        line = jnp.concatenate(lines, axis=0)
        high = line.astype(BF16).astype(F32)
        middle = (line - high).astype(BF16).astype(F32)
        low = line - high - middle
        fill = jnp.zeros((4, 128), F32)
        tail = jnp.concatenate([high, middle, low, fill], axis=0)
        final[target, 2 * rows : 2 * rows + 16, :] = tail.astype(BF16)


def absorb_first(tags, q0, q1, q2, q3, *refs):
    most_out, sums_out = refs[-2:]
    absorb(tags, (q0, q1, q2, q3), refs[:-2], None, None, most_out, sums_out, None)


def absorb_last(tags, q0, q1, q2, q3, most_in, sums_in, *refs):
    absorb(tags, (q0, q1, q2, q3), refs[:-1], most_in, sums_in, None, None, refs[-1])


def finish_heads(tags, parts, lam, gain_a, kept, states, gain_r, keep, give):
    core = tags[0]
    peers = parts.shape[0]
    row = lax.broadcasted_iota(jnp.int32, (128, 128), 0)
    diagonal = row == lax.broadcasted_iota(jnp.int32, (128, 128), 1)
    results = []
    ending = [states[d * 16 : d * 16 + 16].astype(F32).reshape(HG_KEY, HG_KEY).astype(BF16)
              for d in range(2)]
    for n in range(2):
        ratio = []
        for m in range(2):
            k = m * 2 + n
            levels = []
            for p in range(peers):
                tail = parts[p, 512:528, :].astype(F32)
                line = tail[k : k + 1] + tail[k + 4 : k + 5] + tail[k + 8 : k + 9]
                levels.append(jnp.sum(jnp.where(diagonal, line, 0.0), axis=1, keepdims=True))
            top = functools.reduce(jnp.maximum, levels)
            shares = [jnp.exp2(v - top) for v in levels]
            norm = functools.reduce(jnp.add, shares)
            at = slice(k * 128, (k + 1) * 128)
            both = functools.reduce(
                jnp.add, [w * parts[p, at, :].astype(F32) for p, w in enumerate(shares)]
            )
            ratio.append(both / norm)
        diff = ratio[0] - lam[core] * ratio[1]
        mean = jnp.mean(diff * diff, axis=1, keepdims=True)
        attn = (diff * lax.rsqrt(mean + EPSILON) * gain_a[...]).astype(BF16)
        at = slice(n * 128, (n + 1) * 128)
        total = kept[at, :128]
        for d in range(2):
            reach = kept[at, (1 + d) * 128 : (2 + d) * 128].astype(BF16)
            total = total + dot_nt(reach, ending[d])
        mean = jnp.mean(total * total, axis=1, keepdims=True)
        rec = (total * lax.rsqrt(mean + EPSILON) * gain_r[...]).astype(BF16)
        results.append(jnp.concatenate([attn, rec], axis=1))
    keep[...] = jnp.where(core == 0, results[0], results[1])
    give[...] = jnp.where(core == 0, results[1], results[0])


def project_out(tags, keep, got, wa, wr, mixed):
    core = tags[0]
    own = pl.ds(pl.multiple_of(core * 128, 128), 128)
    other = pl.ds(pl.multiple_of((1 - core) * 128, 128), 128)
    result = dot(keep[:, :128], wa[own, :]) + dot(got[:, :128], wa[other, :])
    result = result + dot(keep[:, 128:], wr[own, :]) + dot(got[:, 128:], wr[other, :])
    pieces = mixed.shape[0]
    mixed[...] = result.astype(BF16).reshape(pieces, result.shape[0] // pieces, result.shape[1])


def add_up(parts, out):
    total = functools.reduce(jnp.add, [parts[p].astype(F32) for p in range(parts.shape[0])])
    out[...] = total.astype(BF16)


def local(
    tokens,
    norm_gain,
    da_query,
    da_key,
    da_value,
    mix_lambda,
    attn_gain,
    rec_query,
    rec_forget_fwd,
    rec_forget_bwd,
    rec_value,
    gate_gap,
    extra_decay,
    init_state,
    rec_gain,
    out_attn,
    out_rec,
):
    rows, width = tokens.shape
    tags = jnp.stack(
        [lax.axis_index(C), lax.axis_index(Y), lax.axis_index(X), lax.axis_index((Z, X))]
    ).astype(jnp.int32)

    extra = jnp.transpose(extra_decay, (0, 2, 1)).reshape(4, rows)
    toks = {s: shifted(tokens, Y, s) for s in (2, 1, 3)}
    far = shifted(extra, C, 1)
    mine, theirs = call(
        project,
        [((rows, 7 * 128), BF16)] * 2,
        [
            tags,
            tokens,
            toks[1],
            toks[2],
            toks[3],
            norm_gain.reshape(4, 1, width),
            da_key,
            da_value,
            da_query,
            rec_value,
            rec_query,
            rec_forget_fwd,
            rec_forget_bwd,
        ],
        scratch=[pltpu.VMEM((7, D, 256), BF16), pltpu.SemaphoreType.DMA((7,))],
        specs=[SMEM] + [VMEM] * 5 + [HBM] * 7,
        mib=52,
        flops=2 * rows * D * 7 * 256,
    )
    got = shifted(theirs, C, 1)
    kv, query = call(
        join,
        [((2 * rows, 256), BF16), ((2 * rows, 128), BF16)],
        [tags, mine, got],
        specs=[SMEM, VMEM, VMEM],
    )

    up = shifted(kv, Z, 1)
    down = shifted(kv, Z, 7)
    kept, send = call(
        recurrence_local,
        [((2 * rows, 3 * 128), F32), ((32, 16, 128), BF16)],
        [tags, mine, got, gate_gap, extra, far],
        specs=[SMEM] + [VMEM] * 5,
        flops=2 * rows * 128 * 128 * 40,
    )
    arrived = lax.all_to_all(send, (Z, X), 0, 0, tiled=True)
    up2 = shifted(up, Z, 1)
    down2 = shifted(down, Z, 7)
    queries = {s: shifted(query, X, s) for s in (2, 1, 3)}
    queries = [query] + [queries[s] for s in (1, 2, 3)]
    back = call(
        entering_states,
        ((32, 8, 128), BF16),
        [tags, arrived, init_state.reshape(-1, HG_KEY, HG_KEY)],
        scratch=[pltpu.VMEM((HG_KEY, HG_KEY), F32)],
        specs=[SMEM, VMEM, VMEM],
    )
    up3 = shifted(up2, Z, 1)
    down3 = shifted(down2, Z, 7)
    states = lax.all_to_all(back, (Z, X), 0, 0, tiled=True)
    flops = 4 * 512 * 256 * 2 * 2 * 256
    most, sums = call(
        absorb_first,
        [((4, 4 * rows, 128), F32), ((4, 4 * rows, 256), F32)],
        [tags, *queries, kv, up, down, up2, down2],
        specs=[SMEM] + [VMEM] * 9,
        flops=5 * flops,
        mib=16,
    )
    up4 = shifted(up3, Z, 1)
    parts = call(
        absorb_last,
        ((4, 4 * rows + 16, 128), BF16),
        [tags, *queries, most, sums, up3, down3, up4],
        specs=[SMEM] + [VMEM] * 9,
        flops=3 * flops,
        mib=12,
    )
    parts = lax.all_to_all(parts, X, 0, 0, tiled=True)
    keep, give = call(
        finish_heads,
        [((rows, 256), BF16)] * 2,
        [tags, parts, mix_lambda, attn_gain[None], kept, states, rec_gain[None]],
        specs=[SMEM, VMEM, SMEM] + [VMEM] * 4,
    )
    got = shifted(give, C, 1)
    mixed = call(
        project_out,
        ((4, rows // 4, D), BF16),
        [tags, keep, got, out_attn, out_rec],
        specs=[SMEM] + [VMEM] * 4,
        flops=2 * rows * D * 512,
    )
    mixed = lax.all_to_all(mixed, Y, 0, 0, tiled=True)
    return call(add_up, ((rows // 4, D), BF16), [mixed])


def solution(mesh):
    torus = Mesh(mesh.devices.reshape(8, 4, 2, mesh.shape["tp"]), (Z, X, C, Y))
    return jax.shard_map(
        local,
        mesh=torus,
        in_specs=(
            P(SP, Y),
            P(),
            P(None, Y),
            P(None, Y),
            P(None, Y),
            P(Y),
            P(),
            P(None, Y),
            P(None, Y),
            P(None, Y),
            P(None, Y),
            P(None, Y),
            P(None, SP, Y),
            P(None, Y, None, None),
            P(),
            P(Y, None),
            P(Y, None),
        ),
        out_specs=P((*SP, Y), None),
        check_vma=False,
    )
```

```python
import functools

import jax
import jax.numpy as jnp
from jax import lax
from jax.experimental import pallas as pl
from jax.experimental.pallas import tpu as pltpu
from jax.sharding import Mesh
from jax.sharding import PartitionSpec as P

D = 2048
QK_DIM = 64
HG_KEY = 128
EPSILON = 1e-06
LOG2E = 1.4426950408889634
Z, X, C, Y = ("z", "x", "c", "y")
SP = (Z, X, C)
F32 = jnp.float32
BF16 = jnp.bfloat16


VMEM = pl.BlockSpec(memory_space=pltpu.VMEM)
SMEM = pl.BlockSpec(memory_space=pltpu.SMEM)
HBM = pl.BlockSpec(memory_space=pltpu.HBM)


def call(body, out, ins, scratch=(), specs=None, flops=0, mib=4):
    one = isinstance(out, tuple)
    outs = [out] if one else list(out)
    shapes = [jax.ShapeDtypeStruct(s, t) for s, t in outs]
    specs = specs or [VMEM] * len(ins)
    done = pl.pallas_call(
        body,
        out_shape=shapes,
        in_specs=specs,
        out_specs=[VMEM] * len(shapes),
        scratch_shapes=list(scratch),
        cost_estimate=pl.CostEstimate(flops=flops, transcendentals=0, bytes_accessed=0),
        compiler_params=pltpu.CompilerParams(vmem_limit_bytes=mib << 20),
    )(*ins)
    return done[0] if one else done


def dot(a, b):
    return lax.dot_general(a, b, (((1,), (0,)), ((), ())), preferred_element_type=F32)


def dot_nt(a, b):
    return lax.dot_general(a, b, (((1,), (1,)), ((), ())), preferred_element_type=F32)


def dot_tn(a, b):
    return lax.dot_general(a, b, (((0,), (0,)), ((), ())), preferred_element_type=F32)


def shifted(value, axis, by):
    peers = lax.axis_size(axis)
    return lax.ppermute(value, axis, [(i, (i + by) % peers) for i in range(peers)])


def project(tags, t0, t1, t2, t3, gain, *refs):
    weights = refs[:7]
    mine, theirs, held, sems = refs[7:]
    copies = [
        pltpu.make_async_copy(w, held.at[n], sems.at[n]) for n, w in enumerate(weights)
    ]
    for copy in copies:
        copy.start()
    core = tags[0]
    here = tags[1]
    rows, width = t0.shape
    squares = None
    pieces = []
    starts = []
    for s, tok in enumerate((t0, t1, t2, t3)):
        start = ((here + 4 - s) % 4) * width
        values = tok[...].astype(F32)
        part = jnp.sum(values * values, axis=1, keepdims=True)
        squares = part if squares is None else squares + part
        scale = gain[(here + 4 - s) % 4]
        pieces.append((values * scale).astype(BF16))
        starts.append(pl.multiple_of(start, width))
    inv = lax.rsqrt(squares / (4 * width) + EPSILON)
    for n, copy in enumerate(copies):
        copy.wait()
        total = None
        for piece, start in zip(pieces, starts):
            part = dot(piece, held[n, pl.ds(start, width), :])
            total = part if total is None else total + part
        total = (total * inv).astype(BF16)
        at = slice(n * 128, (n + 1) * 128)
        first = total[:, :128]
        second = total[:, 128:]
        mine[:, at] = jnp.where(core == 0, first, second)
        theirs[:, at] = jnp.where(core == 0, second, first)


def join(tags, mine, got, kv, query):
    core = tags[0]
    rows = mine.shape[0]
    for ref, place in ((mine, core), (got, 1 - core)):
        at = pl.ds(pl.multiple_of(place * rows, rows), rows)
        kv[at, :] = ref[:, :256]
        query[at, :] = ref[:, 256:384]


def triangle_sum(ones, value):
    high = value.astype(BF16)
    rest = value - high.astype(F32)
    middle = rest.astype(BF16)
    low = (rest - middle.astype(F32)).astype(BF16)
    return dot(ones, high) + dot(ones, middle) + dot(ones, low)


def recurrence_local(tags, mine, got, gap, extra, far, kept, send):
    core = tags[0]
    rows = mine.shape[0]
    row = lax.broadcasted_iota(jnp.int32, (rows, rows), 0)
    col = lax.broadcasted_iota(jnp.int32, (rows, rows), 1)
    sub = lax.broadcasted_iota(jnp.int32, (8, HG_KEY), 0)
    a = mine[:, 384:]
    b = got[:, 384:]
    blocks = (jnp.where(core == 0, a, b), jnp.where(core == 0, b, a))
    values = [x[:, :128] for x in blocks]
    rec_q = []
    for x in blocks:
        rq = x[:, 128:256].astype(F32)
        rec_q.append(rq / (1.0 + jnp.exp(-rq)) * HG_KEY**-0.5)
    out = [None, None]
    pieces = HG_KEY // 8
    for d in range(2):
        keep = (row >= col) if d == 0 else (row <= col)
        ones = keep.astype(BF16)
        pair = gap[d : d + 1, :]
        share = jnp.where(core == 0, pair[:, :128], pair[:, 128:])
        order = (0, 1) if d == 0 else (1, 0)
        state = None
        before = None
        for n in order:
            forget = blocks[n][:, (2 + d) * 128 : (3 + d) * 128].astype(F32)
            key = share / (1.0 + jnp.exp(forget))
            mine_line = extra[d * 2 : d * 2 + 1, :]
            got_line = far[d * 2 : d * 2 + 1, :]
            line0 = jnp.where(core == n, mine_line, got_line)
            mine_line = extra[d * 2 + 1 : d * 2 + 2, :]
            got_line = far[d * 2 + 1 : d * 2 + 2, :]
            line1 = jnp.where(core == n, mine_line, got_line)
            line = jnp.where(core == 0, line0, line1)
            more = jnp.sum(jnp.where(keep, line, 0.0), axis=1, keepdims=True)
            total = triangle_sum(ones, jnp.log1p(-key)) + more
            last = rows - 1 if d == 0 else 0
            end = total[last : last + 1, :]
            middle = total[rows // 2 : rows // 2 + 1, :]
            near_q = (rec_q[n] * jnp.exp(total - middle)).astype(BF16)
            near_k = (key * jnp.exp(middle - total)).astype(BF16)
            score = jnp.where(keep, dot_nt(near_q, near_k), 0.0).astype(BF16)
            result = dot(score, values[n])
            far_k = (key * jnp.exp(end - total)).astype(BF16)
            piece = dot_tn(values[n], far_k)
            if state is None:
                state = piece
                before = end
                reach = total
            else:
                near = (rec_q[n] * jnp.exp(total)).astype(BF16)
                result = result + dot_nt(near, state.astype(BF16))
                state = jnp.exp(end) * state + piece
                reach = total + before
                before = before + end
            kept[n * rows : (n + 1) * rows, (1 + d) * 128 : (2 + d) * 128] = rec_q[n] * jnp.exp(
                reach
            )
            out[n] = result if out[n] is None else out[n] + result
        high = before.astype(BF16).astype(F32)
        low = before - high
        tail = jnp.where(sub == 0, high, jnp.where(sub == 1, low, 0.0))
        tail = jnp.broadcast_to(tail[None], (pieces, 8, HG_KEY))
        both = jnp.concatenate([state.reshape(pieces, 8, HG_KEY), tail], axis=1)
        send[d * pieces : (d + 1) * pieces] = both.astype(BF16)
    for n in range(2):
        kept[n * rows : (n + 1) * rows, :128] = out[n]


def entering_states(tags, got, init, send, turned):
    me = tags[3]
    peers = got.shape[0]
    pieces = HG_KEY // 8
    which = (me // pieces) * 2 + tags[0]
    turned[...] = init[which].T
    state = turned[pl.ds(pl.multiple_of((me % pieces) * 8, 8), 8), :]
    backward = me >= peers // 2
    for t in range(peers):
        at = jnp.where(backward, peers - 1 - t, t)
        send[at] = state.astype(BF16)
        piece = got[at].astype(F32)
        decay = piece[8:9, :] + piece[9:10, :]
        state = jnp.exp(decay) * state + piece[:8, :]


def absorb(tags, queries, pieces, most_in, sums_in, most_out, sums_out, final):
    rows = queries[0].shape[0]
    lane = lax.broadcasted_iota(jnp.int32, (rows, 128), 1)
    row = lax.broadcasted_iota(jnp.int32, (128, 128), 0)
    diagonal = row == lax.broadcasted_iota(jnp.int32, (128, 128), 1)
    scale = QK_DIM**-0.5 * LOG2E
    key = jnp.concatenate([p[:, :128] for p in pieces], axis=0)
    val = jnp.concatenate([p[:, 128:] for p in pieces], axis=0)
    val = jnp.concatenate([val, jnp.ones(val.shape, BF16)], axis=1)
    for s, q in enumerate(queries):
        query = q[...]
        none = jnp.zeros_like(query)
        both = jnp.concatenate(
            [jnp.where(lane < QK_DIM, query, none), jnp.where(lane < QK_DIM, none, query)],
            axis=0,
        )
        score = dot_nt(both, key)
        most = jnp.max(score, axis=1, keepdims=True)
        if most_in is not None:
            old = most_in[s][:, :1]
            most = jnp.maximum(most, old)
        weight = jnp.exp2((score - most) * scale).astype(BF16)
        sums = dot(weight, val)
        if most_in is not None:
            sums = sums + jnp.exp2((old - most) * scale) * sums_in[s]
        if final is None:
            most_out[s] = jnp.broadcast_to(most, (2 * rows, 128))
            sums_out[s] = sums
            continue
        where = (tags[2] + 4 - s) % 4
        norm = sums[:, 128:]
        share = (sums[:, :128] / norm).astype(BF16)
        level = most * scale + jnp.log2(norm)
        for n in range(2):
            target = where * 2 + n
            lines = []
            for m in range(2):
                at = slice(m * rows + n * 128, m * rows + (n + 1) * 128)
                final[target, m * 128 : (m + 1) * 128, :] = share[at]
                lines.append(jnp.sum(jnp.where(diagonal, level[at], 0.0), 0, keepdims=True))
            line = jnp.concatenate(lines, axis=0)
            high = line.astype(BF16).astype(F32)
            middle = (line - high).astype(BF16).astype(F32)
            low = line - high - middle
            fill = jnp.zeros((10, 128), F32)
            tail = jnp.concatenate([high, middle, low, fill], axis=0)
            final[target, 256:272, :] = tail.astype(BF16)


def absorb_first(tags, q0, q1, q2, q3, *refs):
    most_out, sums_out = refs[-2:]
    absorb(tags, (q0, q1, q2, q3), refs[:-2], None, None, most_out, sums_out, None)


def absorb_last(tags, q0, q1, q2, q3, most_in, sums_in, *refs):
    absorb(tags, (q0, q1, q2, q3), refs[:-1], most_in, sums_in, None, None, refs[-1])


def finish_recurrence(tags, kept, states, gain, keep, give):
    core = tags[0]
    results = []
    ending = [
        states[d * 16 : d * 16 + 16].astype(F32).reshape(HG_KEY, HG_KEY).astype(BF16)
        for d in range(2)
    ]
    for n in range(2):
        at = slice(n * 128, (n + 1) * 128)
        total = kept[at, :128]
        for d in range(2):
            reach = kept[at, (1 + d) * 128 : (2 + d) * 128].astype(BF16)
            total = total + dot_nt(reach, ending[d])
        mean = jnp.mean(total * total, axis=1, keepdims=True)
        results.append((total * lax.rsqrt(mean + EPSILON) * gain[...]).astype(BF16))
    keep[...] = jnp.where(core == 0, results[0], results[1])
    give[...] = jnp.where(core == 0, results[1], results[0])


def finish(tags, parts, lam, gain, keep, got, wa, wr, mixed):
    core = tags[0]
    peers = parts.shape[0] // 2
    row = lax.broadcasted_iota(jnp.int32, (128, 128), 0)
    diagonal = row == lax.broadcasted_iota(jnp.int32, (128, 128), 1)
    heads = []
    for h in range(2):
        ratio = []
        for m in range(2):
            levels = []
            for p in range(peers):
                tail = parts[p * 2 + h, 256:272, :].astype(F32)
                line = tail[m : m + 1] + tail[m + 2 : m + 3] + tail[m + 4 : m + 5]
                levels.append(jnp.sum(jnp.where(diagonal, line, 0.0), axis=1, keepdims=True))
            top = functools.reduce(jnp.maximum, levels)
            shares = [jnp.exp2(v - top) for v in levels]
            norm = functools.reduce(jnp.add, shares)
            at = slice(m * 128, (m + 1) * 128)
            both = functools.reduce(
                jnp.add,
                [w * parts[p * 2 + h, at, :].astype(F32) for p, w in enumerate(shares)],
            )
            ratio.append(both / norm)
        diff = ratio[0] - lam[h] * ratio[1]
        mean = jnp.mean(diff * diff, axis=1, keepdims=True)
        heads.append((diff * lax.rsqrt(mean + EPSILON) * gain[...]).astype(BF16))
    own = pl.ds(pl.multiple_of(core * 128, 128), 128)
    other = pl.ds(pl.multiple_of((1 - core) * 128, 128), 128)
    result = dot(keep[...], wr[own, :]) + dot(got[...], wr[other, :])
    result = result + dot(jnp.concatenate(heads, axis=1), wa[...])
    pieces = mixed.shape[0]
    mixed[...] = result.astype(BF16).reshape(pieces, result.shape[0] // pieces, result.shape[1])


def add_up(parts, out):
    total = functools.reduce(jnp.add, [parts[p].astype(F32) for p in range(parts.shape[0])])
    out[...] = total.astype(BF16)


def local(
    tokens,
    norm_gain,
    da_query,
    da_key,
    da_value,
    mix_lambda,
    attn_gain,
    rec_query,
    rec_forget_fwd,
    rec_forget_bwd,
    rec_value,
    gate_gap,
    extra_decay,
    init_state,
    rec_gain,
    out_attn,
    out_rec,
):
    rows, width = tokens.shape
    tags = jnp.stack(
        [lax.axis_index(C), lax.axis_index(Y), lax.axis_index(X), lax.axis_index((Z, X))]
    ).astype(jnp.int32)

    extra = jnp.transpose(extra_decay, (0, 2, 1)).reshape(4, rows)
    toks = {s: shifted(tokens, Y, s) for s in (2, 1, 3)}
    far = shifted(extra, C, 1)
    mine, theirs = call(
        project,
        [((rows, 7 * 128), BF16)] * 2,
        [
            tags,
            tokens,
            toks[1],
            toks[2],
            toks[3],
            norm_gain.reshape(4, 1, width),
            da_key,
            da_value,
            da_query,
            rec_value,
            rec_query,
            rec_forget_fwd,
            rec_forget_bwd,
        ],
        scratch=[pltpu.VMEM((7, D, 256), BF16), pltpu.SemaphoreType.DMA((7,))],
        specs=[SMEM] + [VMEM] * 5 + [HBM] * 7,
        mib=52,
        flops=2 * rows * D * 7 * 256,
    )
    got = shifted(theirs, C, 1)
    kv, query = call(
        join,
        [((2 * rows, 256), BF16), ((2 * rows, 128), BF16)],
        [tags, mine, got],
        specs=[SMEM, VMEM, VMEM],
    )

    up = shifted(kv, Z, 1)
    down = shifted(kv, Z, 7)
    kept, send = call(
        recurrence_local,
        [((2 * rows, 3 * 128), F32), ((32, 16, 128), BF16)],
        [tags, mine, got, gate_gap, extra, far],
        specs=[SMEM] + [VMEM] * 5,
        flops=2 * rows * 128 * 128 * 40,
    )
    arrived = lax.all_to_all(send, (Z, X), 0, 0, tiled=True)
    up2 = shifted(up, Z, 1)
    down2 = shifted(down, Z, 7)
    queries = {s: shifted(query, X, s) for s in (2, 1, 3)}
    queries = [query] + [queries[s] for s in (1, 2, 3)]
    back = call(
        entering_states,
        ((32, 8, 128), BF16),
        [tags, arrived, init_state.reshape(-1, HG_KEY, HG_KEY)],
        scratch=[pltpu.VMEM((HG_KEY, HG_KEY), F32)],
        specs=[SMEM, VMEM, VMEM],
    )
    up3 = shifted(up2, Z, 1)
    down3 = shifted(down2, Z, 7)
    states = lax.all_to_all(back, (Z, X), 0, 0, tiled=True)
    flops = 4 * 512 * 256 * 2 * 2 * 256
    most, sums = call(
        absorb_first,
        [((4, 4 * rows, 128), F32), ((4, 4 * rows, 256), F32)],
        [tags, *queries, kv, up, down, up2, down2],
        specs=[SMEM] + [VMEM] * 9,
        flops=5 * flops,
        mib=16,
    )
    up4 = shifted(up3, Z, 1)
    parts = call(
        absorb_last,
        ((8, 2 * rows + 16, 128), BF16),
        [tags, *queries, most, sums, up3, down3, up4],
        specs=[SMEM] + [VMEM] * 9,
        flops=3 * flops,
        mib=12,
    )
    keep, give = call(
        finish_recurrence,
        [((rows, 128), BF16)] * 2,
        [tags, kept, states, rec_gain[None]],
        specs=[SMEM] + [VMEM] * 3,
    )
    got = shifted(give, C, 1)
    parts = lax.all_to_all(parts, (X, C), 0, 0, tiled=True)
    mixed = call(
        finish,
        ((4, rows // 4, D), BF16),
        [tags, parts, mix_lambda, attn_gain[None], keep, got, out_attn, out_rec],
        specs=[SMEM, VMEM, SMEM] + [VMEM] * 5,
        flops=2 * rows * D * 512,
    )
    mixed = lax.all_to_all(mixed, Y, 0, 0, tiled=True)
    return call(add_up, ((rows // 4, D), BF16), [mixed])


def solution(mesh):
    torus = Mesh(mesh.devices.reshape(8, 4, 2, mesh.shape["tp"]), (Z, X, C, Y))
    return jax.shard_map(
        local,
        mesh=torus,
        in_specs=(
            P(SP, Y),
            P(),
            P(None, Y),
            P(None, Y),
            P(None, Y),
            P(Y),
            P(),
            P(None, Y),
            P(None, Y),
            P(None, Y),
            P(None, Y),
            P(None, Y),
            P(None, SP, Y),
            P(None, Y, None, None),
            P(),
            P(Y, None),
            P(Y, None),
        ),
        out_specs=P((*SP, Y), None),
        check_vma=False,
    )
```

```python
import functools

import jax
import jax.numpy as jnp
from jax import lax
from jax.experimental import pallas as pl
from jax.experimental.pallas import tpu as pltpu
from jax.sharding import Mesh
from jax.sharding import PartitionSpec as P


D = 2048
QK_DIM = 64
HG_KEY = 128
EPSILON = 1e-06
LOG2E = 1.4426950408889634
Z, X, C, Y = ("z", "x", "c", "y")
SP = (Z, X, C)
F32 = jnp.float32
BF16 = jnp.bfloat16


VMEM = pl.BlockSpec(memory_space=pltpu.VMEM)
SMEM = pl.BlockSpec(memory_space=pltpu.SMEM)
HBM = pl.BlockSpec(memory_space=pltpu.HBM)


def call(body, out, ins, scratch=(), specs=None, flops=0, mib=4, outs_at=None, aliases=None):
    one = isinstance(out, tuple)
    outs = [out] if one else list(out)
    shapes = [jax.ShapeDtypeStruct(s, t) for s, t in outs]
    specs = specs or [VMEM] * len(ins)
    done = pl.pallas_call(
        body,
        out_shape=shapes,
        in_specs=specs,
        out_specs=outs_at or [VMEM] * len(shapes),
        input_output_aliases=aliases or {},
        scratch_shapes=list(scratch),
        cost_estimate=pl.CostEstimate(flops=flops, transcendentals=0, bytes_accessed=0),
        compiler_params=pltpu.CompilerParams(vmem_limit_bytes=mib << 20),
    )(*ins)
    return done[0] if one else done


def dot(a, b):
    return lax.dot_general(a, b, (((1,), (0,)), ((), ())), preferred_element_type=F32)


def dot_nt(a, b):
    return lax.dot_general(a, b, (((1,), (1,)), ((), ())), preferred_element_type=F32)


def dot_tn(a, b):
    return lax.dot_general(a, b, (((0,), (0,)), ((), ())), preferred_element_type=F32)


def shifted(value, axis, by):
    peers = lax.axis_size(axis)
    return lax.ppermute(value, axis, [(i, (i + by) % peers) for i in range(peers)])


def fetch(tokens, gain, own, gain_out, sems):
    copies = [
        pltpu.make_async_copy(tokens, own, sems.at[0]),
        pltpu.make_async_copy(gain, gain_out, sems.at[1]),
    ]
    for copy in copies:
        copy.start()
    for copy in copies:
        copy.wait()


def project(tags, t0, t1, t2, t3, gain, *refs):
    weights = refs[:7]
    mine, theirs, held, sems = refs[7:]
    copies = [
        pltpu.make_async_copy(w, held.at[n], sems.at[n]) for n, w in enumerate(weights)
    ]
    ahead = 3
    for copy in copies[:ahead]:
        copy.start()
    core = tags[0]
    here = tags[1]
    _, width = t0.shape
    squares = None
    pieces = []
    starts = []
    for s, tok in enumerate((t0, t1, t2, t3)):
        start = ((here + 4 - s) % 4) * width
        values = tok[...].astype(F32)
        part = jnp.sum(values * values, axis=1, keepdims=True)
        squares = part if squares is None else squares + part
        scale = gain[(here + 4 - s) % 4]
        pieces.append((values * scale).astype(BF16))
        starts.append(pl.multiple_of(start, width))
    inv = lax.rsqrt(squares / (4 * width) + EPSILON)
    for n, copy in enumerate(copies):
        copy.wait()
        if n + ahead < len(copies):
            copies[n + ahead].start()
        total = None
        for piece, start in zip(pieces, starts):
            part = dot(piece, held[n, pl.ds(start, width), :])
            total = part if total is None else total + part
        total = (total * inv).astype(BF16)
        at = slice(n * 128, (n + 1) * 128)
        first = total[:, :128]
        second = total[:, 128:]
        mine[:, at] = jnp.where(core == 0, first, second)
        theirs[:, at] = jnp.where(core == 0, second, first)


def join(tags, mine, got, kv, query):
    core = tags[0]
    rows = mine.shape[0]
    for ref, place in ((mine, core), (got, 1 - core)):
        at = pl.ds(pl.multiple_of(place * rows, rows), rows)
        kv[at, :] = ref[:, :256]
        query[at, :] = ref[:, 256:384]


def triangle_sum(ones, value):
    high = value.astype(BF16)
    rest = value - high.astype(F32)
    middle = rest.astype(BF16)
    low = (rest - middle.astype(F32)).astype(BF16)
    return dot(ones, high) + dot(ones, middle) + dot(ones, low)


def recurrence_local(tags, mine, got, gap, extra, far, kept, send):
    core = tags[0]
    rows = mine.shape[0]
    row = lax.broadcasted_iota(jnp.int32, (rows, rows), 0)
    col = lax.broadcasted_iota(jnp.int32, (rows, rows), 1)
    sub = lax.broadcasted_iota(jnp.int32, (8, HG_KEY), 0)
    a = mine[:, 384:]
    b = got[:, 384:]
    blocks = (jnp.where(core == 0, a, b), jnp.where(core == 0, b, a))
    values = [x[:, :128] for x in blocks]
    rec_q = []
    for x in blocks:
        rq = x[:, 128:256].astype(F32)
        rec_q.append(rq / (1.0 + jnp.exp(-rq)) * HG_KEY**-0.5)
    out = [None, None]
    pieces = HG_KEY // 8
    for d in range(2):
        keep = (row >= col) if d == 0 else (row <= col)
        ones = keep.astype(BF16)
        pair = gap[d : d + 1, :]
        share = jnp.where(core == 0, pair[:, :128], pair[:, 128:])
        order = (0, 1) if d == 0 else (1, 0)
        state = None
        before = None
        for n in order:
            forget = blocks[n][:, (2 + d) * 128 : (3 + d) * 128].astype(F32)
            key = share / (1.0 + jnp.exp(forget))
            mine_line = extra[d * 2 : d * 2 + 1, :]
            got_line = far[d * 2 : d * 2 + 1, :]
            line0 = jnp.where(core == n, mine_line, got_line)
            mine_line = extra[d * 2 + 1 : d * 2 + 2, :]
            got_line = far[d * 2 + 1 : d * 2 + 2, :]
            line1 = jnp.where(core == n, mine_line, got_line)
            line = jnp.where(core == 0, line0, line1)
            more = jnp.sum(jnp.where(keep, line, 0.0), axis=1, keepdims=True)
            total = triangle_sum(ones, jnp.log1p(-key)) + more
            last = rows - 1 if d == 0 else 0
            end = total[last : last + 1, :]
            middle = total[rows // 2 : rows // 2 + 1, :]
            near_q = (rec_q[n] * jnp.exp(total - middle)).astype(BF16)
            near_k = (key * jnp.exp(middle - total)).astype(BF16)
            score = jnp.where(keep, dot_nt(near_q, near_k), 0.0).astype(BF16)
            result = dot(score, values[n])
            far_k = (key * jnp.exp(end - total)).astype(BF16)
            piece = dot_tn(values[n], far_k)
            if state is None:
                state = piece
                before = end
                reach = total
            else:
                near = (rec_q[n] * jnp.exp(total)).astype(BF16)
                result = result + dot_nt(near, state.astype(BF16))
                state = jnp.exp(end) * state + piece
                reach = total + before
                before = before + end
            kept[n * rows : (n + 1) * rows, (1 + d) * 128 : (2 + d) * 128] = rec_q[n] * jnp.exp(
                reach
            )
            out[n] = result if out[n] is None else out[n] + result
        high = before.astype(BF16).astype(F32)
        low = before - high
        tail = jnp.where(sub == 0, high, jnp.where(sub == 1, low, 0.0))
        tail = jnp.broadcast_to(tail[None], (pieces, 8, HG_KEY))
        both = jnp.concatenate([state.reshape(pieces, 8, HG_KEY), tail], axis=1)
        send[d * pieces : (d + 1) * pieces] = both.astype(BF16)
    for n in range(2):
        kept[n * rows : (n + 1) * rows, :128] = out[n]


def entering_states(tags, got, init, send, turned):
    me = tags[3]
    peers = got.shape[0]
    pieces = HG_KEY // 8
    which = (me // pieces) * 2 + tags[0]
    turned[...] = init[which].T
    state = turned[pl.ds(pl.multiple_of((me % pieces) * 8, 8), 8), :]
    backward = me >= peers // 2
    for t in range(peers):
        at = jnp.where(backward, peers - 1 - t, t)
        send[at] = state.astype(BF16)
        piece = got[at].astype(F32)
        decay = piece[8:9, :] + piece[9:10, :]
        state = jnp.exp(decay) * state + piece[:8, :]


def absorb(
    tags, queries, pieces, most_in, sums_in, most_out, sums_out, final, lam=None
):
    rows = queries[0].shape[0]
    lane = lax.broadcasted_iota(jnp.int32, (rows, 128), 1)
    row = lax.broadcasted_iota(jnp.int32, (128, 128), 0)
    diagonal = row == lax.broadcasted_iota(jnp.int32, (128, 128), 1)
    scale = QK_DIM**-0.5 * LOG2E
    key = jnp.concatenate([p[:, :128] for p in pieces], axis=0)
    val = jnp.concatenate([p[:, 128:] for p in pieces], axis=0)
    val = jnp.concatenate([val, jnp.ones(val.shape, BF16)], axis=1)
    for s, q in enumerate(queries):
        query = q[...]
        none = jnp.zeros_like(query)
        both = jnp.concatenate(
            [jnp.where(lane < QK_DIM, query, none), jnp.where(lane < QK_DIM, none, query)],
            axis=0,
        )
        score = dot_nt(both, key)
        most = jnp.max(score, axis=1, keepdims=True)
        if most_in is not None:
            old = most_in[s][:, :1]
            most = jnp.maximum(most, old)
        weight = jnp.exp2((score - most) * scale).astype(BF16)
        sums = dot(weight, val)
        if most_in is not None:
            sums = sums + jnp.exp2((old - most) * scale) * sums_in[s]
        if final is None:
            most_out[s] = jnp.broadcast_to(most, (2 * rows, 128))
            sums_out[s] = sums
            continue
        where = (tags[2] + 4 - s) % 4
        norm = sums[:, 128:]
        share = sums[:, :128] / norm
        share = jnp.concatenate([share[:rows], share[rows:] * lam], axis=0).astype(BF16)
        level = most * scale + jnp.log2(norm)
        for n in range(4):
            target = where * 4 + n
            cuts = [slice(k * 128 + n * 32, k * 128 + (n + 1) * 32) for k in range(4)]
            final[target, :128, :] = jnp.concatenate([share[at] for at in cuts], axis=0)
            column = jnp.concatenate([level[at] for at in cuts], axis=0)
            line = jnp.sum(jnp.where(diagonal, column, 0.0), 0, keepdims=True)
            high = line.astype(BF16).astype(F32)
            middle = (line - high).astype(BF16).astype(F32)
            low = line - high - middle
            tail = jnp.concatenate([high, middle, low, jnp.zeros((13, 128), F32)], axis=0)
            final[target, 128:144, :] = tail.astype(BF16)


def absorb_first(tags, q0, q1, q2, q3, *refs):
    most_out, sums_out = refs[-2:]
    absorb(tags, (q0, q1, q2, q3), refs[:-2], None, None, most_out, sums_out, None)


def absorb_last(tags, lam, q0, q1, q2, q3, most_in, sums_in, *refs):
    absorb(
        tags,
        (q0, q1, q2, q3),
        refs[:-1],
        most_in,
        sums_in,
        None,
        None,
        refs[-1],
        lam[tags[0]],
    )


def finish_recurrence(tags, kept, states, gain, parts, out, held, sems):
    ending = [
        states[d * 16 : d * 16 + 16].astype(F32).reshape(HG_KEY, HG_KEY).astype(BF16)
        for d in range(2)
    ]
    total = kept[:, :128]
    for d in range(2):
        reach = kept[:, (1 + d) * 128 : (2 + d) * 128].astype(BF16)
        total = total + dot_nt(reach, ending[d])
    mean = jnp.mean(total * total, axis=1, keepdims=True)
    rec = (total * lax.rsqrt(mean + EPSILON) * gain[...]).astype(BF16)
    copies = []
    for n in range(4):
        held[n, :32, :] = rec[n * 32 : (n + 1) * 32]
        held[n, 32:, :] = rec[128 + n * 32 : 128 + (n + 1) * 32]
        copies.append(
            pltpu.make_async_copy(
                held.at[n], out.at[tags[2] * 4 + n, pl.ds(144, 64), :], sems.at[n]
            )
        )
    for copy in copies:
        copy.start()
    for copy in copies:
        copy.wait()


def finish(tags, parts, gain, *refs):
    weights = refs[:8]
    keep, give, held, sems = refs[8:]
    copies = [
        pltpu.make_async_copy(
            weights[h * 4 + s], held.at[s, pl.ds(h * 128, 128), :], sems.at[s * 2 + h]
        )
        for s in range(4)
        for h in range(2)
    ]
    for copy in copies:
        copy.start()
    core = tags[0]
    row = lax.broadcasted_iota(jnp.int32, (128, 128), 0)
    diagonal = row == lax.broadcasted_iota(jnp.int32, (128, 128), 1)
    result = None
    for s in range(4):
        head = (tags[1] + 4 - s) % 4
        levels = []
        for p in range(4):
            tail = parts[p * 4 + head, 128:144, :].astype(F32)
            line = tail[0:1] + tail[1:2] + tail[2:3]
            levels.append(jnp.sum(jnp.where(diagonal, line, 0.0), axis=1, keepdims=True))
        top = functools.reduce(jnp.maximum, levels)
        shares = [jnp.exp2(v - top) for v in levels]
        norm = functools.reduce(jnp.add, shares)
        both = functools.reduce(
            jnp.add, [w * parts[p * 4 + head, :128, :].astype(F32) for p, w in enumerate(shares)]
        )
        both = both / norm
        diff = both[:64] - both[64:]
        mean = jnp.mean(diff * diff, axis=1, keepdims=True)
        attn = (diff * lax.rsqrt(mean + EPSILON) * gain[...]).astype(BF16)
        rec = parts[tags[2] * 4 + head, 144:208, :]
        copies[s * 2].wait()
        copies[s * 2 + 1].wait()
        part = dot(jnp.concatenate([attn, rec], axis=1), held[s])
        result = part if result is None else result + part
    keep[...] = jnp.where(core == 0, result[:32], result[32:])
    give[...] = jnp.where(core == 0, result[32:], result[:32]).astype(BF16)


def add_up(keep, got, out):
    out[...] = (keep[...] + got[...].astype(F32)).astype(BF16)


def local(
    tokens,
    norm_gain,
    da_query,
    da_key,
    da_value,
    mix_lambda,
    attn_gain,
    rec_query,
    rec_forget_fwd,
    rec_forget_bwd,
    rec_value,
    gate_gap,
    extra_decay,
    init_state,
    rec_gain,
    out_attn,
    out_rec,
):
    rows, width = tokens.shape
    tags = jnp.stack(
        [lax.axis_index(C), lax.axis_index(Y), lax.axis_index(X), lax.axis_index((Z, X))]
    ).astype(jnp.int32)

    extra = jnp.transpose(extra_decay, (0, 2, 1)).reshape(4, rows)
    toks = {s: shifted(tokens, Y, s) for s in (2, 1, 3)}
    far = shifted(extra, C, 1)
    own, gain = call(
        fetch,
        [((rows, width), BF16), ((4, 1, width), F32)],
        [tokens, norm_gain.reshape(4, 1, width)],
        scratch=[pltpu.SemaphoreType.DMA((2,))],
        specs=[HBM] * 2,
        flops=1 << 30,
        mib=52,
    )
    first = lax.axis_index(C) * 128
    attn_own = lax.dynamic_slice_in_dim(out_attn, first, 128, axis=0)
    rec_own = lax.dynamic_slice_in_dim(out_rec, first, 128, axis=0)
    attn_up = shifted(attn_own, Y, 1)
    attn_down = shifted(attn_own, Y, 3)
    rec_up = shifted(rec_own, Y, 1)
    rec_down = shifted(rec_own, Y, 3)
    attn_rows = [attn_own, attn_up, shifted(attn_up, Y, 1), attn_down]
    rec_rows = [rec_own, rec_up, shifted(rec_down, Y, 3), rec_down]
    mine, theirs = call(
        project,
        [((rows, 7 * 128), BF16)] * 2,
        [
            tags,
            own,
            toks[1],
            toks[2],
            toks[3],
            gain,
            da_key,
            da_value,
            da_query,
            rec_value,
            rec_query,
            rec_forget_fwd,
            rec_forget_bwd,
        ],
        scratch=[pltpu.VMEM((7, D, 256), BF16), pltpu.SemaphoreType.DMA((7,))],
        specs=[SMEM] + [VMEM] * 5 + [HBM] * 7,
        mib=52,
        flops=2 * rows * D * 7 * 256,
    )
    got = shifted(theirs, C, 1)
    kv, query = call(
        join,
        [((2 * rows, 256), BF16), ((2 * rows, 128), BF16)],
        [tags, mine, got],
        specs=[SMEM, VMEM, VMEM],
    )

    up = shifted(kv, Z, 1)
    down = shifted(kv, Z, 7)
    kept, send = call(
        recurrence_local,
        [((2 * rows, 3 * 128), F32), ((32, 16, 128), BF16)],
        [tags, mine, got, gate_gap, extra, far],
        specs=[SMEM] + [VMEM] * 5,
        flops=2 * rows * 128 * 128 * 40,
    )
    arrived = lax.all_to_all(send, (Z, X), 0, 0, tiled=True)
    up2 = shifted(up, Z, 1)
    down2 = shifted(down, Z, 7)
    queries = {s: shifted(query, X, s) for s in (2, 1, 3)}
    queries = [query] + [queries[s] for s in (1, 2, 3)]
    back = call(
        entering_states,
        ((32, 8, 128), BF16),
        [tags, arrived, init_state.reshape(-1, HG_KEY, HG_KEY)],
        scratch=[pltpu.VMEM((HG_KEY, HG_KEY), F32)],
        specs=[SMEM, VMEM, VMEM],
    )
    up3 = shifted(up2, Z, 1)
    down3 = shifted(down2, Z, 7)
    states = lax.all_to_all(back, (Z, X), 0, 0, tiled=True)
    flops = 4 * 512 * 256 * 2 * 2 * 256
    most, sums = call(
        absorb_first,
        [((4, 4 * rows, 128), F32), ((4, 4 * rows, 256), F32)],
        [tags, *queries, kv, up, down, up2, down2],
        specs=[SMEM] + [VMEM] * 9,
        flops=5 * flops,
        mib=16,
    )
    up4 = shifted(up3, Z, 1)
    parts = call(
        absorb_last,
        ((16, 208, 128), BF16),
        [
            tags,
            mix_lambda,
            *queries,
            most,
            sums,
            up3,
            down3,
            up4,
        ],
        specs=[SMEM, SMEM] + [VMEM] * 9,
        flops=3 * flops,
        mib=12,
    )
    parts = call(
        finish_recurrence,
        ((16, 208, 128), BF16),
        [tags, kept, states, rec_gain[None], parts],
        scratch=[pltpu.VMEM((4, 64, 128), BF16), pltpu.SemaphoreType.DMA((4,))],
        specs=[SMEM] + [VMEM] * 3 + [HBM],
        outs_at=[HBM],
        aliases={4: 0},
    )
    parts = lax.all_to_all(parts, (X, Y), 0, 0, tiled=True)
    keep, give = call(
        finish,
        [((rows // 4, D), F32), ((rows // 4, D), BF16)],
        [tags, parts, attn_gain[None], *attn_rows, *rec_rows],
        scratch=[pltpu.VMEM((4, 256, D), BF16), pltpu.SemaphoreType.DMA((8,))],
        specs=[SMEM, VMEM, VMEM] + [HBM] * 8,
        flops=2 * 64 * D * 1024,
        mib=52,
    )
    got = shifted(give, C, 1)
    return call(add_up, ((rows // 4, D), BF16), [keep, got])


def solution(mesh):
    torus = Mesh(mesh.devices.reshape(8, 4, 2, mesh.shape["tp"]), (Z, X, C, Y))
    return jax.shard_map(
        local,
        mesh=torus,
        in_specs=(
            P(SP, Y),
            P(),
            P(None, Y),
            P(None, Y),
            P(None, Y),
            P(Y),
            P(),
            P(None, Y),
            P(None, Y),
            P(None, Y),
            P(None, Y),
            P(None, Y),
            P(None, SP, Y),
            P(None, Y, None, None),
            P(),
            P(Y, None),
            P(Y, None),
        ),
        out_specs=P((*SP, Y), None),
        check_vma=False,
    )
```

```python
import functools

import jax
import jax.numpy as jnp
from jax import lax
from jax.experimental import pallas as pl
from jax.experimental.pallas import tpu as pltpu
from jax.sharding import Mesh
from jax.sharding import PartitionSpec as P

D = 2048
QK_DIM = 64
HG_KEY = 128
EPSILON = 1e-06
LOG2E = 1.4426950408889634
Z, X, C, Y = ("z", "x", "c", "y")
SP = (Z, X, C)
F32 = jnp.float32
BF16 = jnp.bfloat16


VMEM = pl.BlockSpec(memory_space=pltpu.VMEM)
SMEM = pl.BlockSpec(memory_space=pltpu.SMEM)
HBM = pl.BlockSpec(memory_space=pltpu.HBM)


def call(body, out, ins, scratch=(), specs=None, flops=0, mib=4):
    one = isinstance(out, tuple)
    outs = [out] if one else list(out)
    shapes = [jax.ShapeDtypeStruct(s, t) for s, t in outs]
    specs = specs or [VMEM] * len(ins)
    done = pl.pallas_call(
        body,
        out_shape=shapes,
        in_specs=specs,
        out_specs=[VMEM] * len(shapes),
        scratch_shapes=list(scratch),
        cost_estimate=pl.CostEstimate(flops=flops, transcendentals=0, bytes_accessed=0),
        compiler_params=pltpu.CompilerParams(vmem_limit_bytes=mib << 20),
    )(*ins)
    return done[0] if one else done


def dot(a, b):
    return lax.dot_general(a, b, (((1,), (0,)), ((), ())), preferred_element_type=F32)


def dot_nt(a, b):
    return lax.dot_general(a, b, (((1,), (1,)), ((), ())), preferred_element_type=F32)


def dot_tn(a, b):
    return lax.dot_general(a, b, (((0,), (0,)), ((), ())), preferred_element_type=F32)


def shifted(value, axis, by):
    peers = lax.axis_size(axis)
    return lax.ppermute(value, axis, [(i, (i + by) % peers) for i in range(peers)])


def begin(tags, tokens, gain, *refs):
    weights = refs[:7]
    partial, gain_out, squares, own, held, sems = refs[7:]
    width = tokens.shape[1]
    at = pl.ds(pl.multiple_of(tags[1] * width, width), width)
    copies = [
        pltpu.make_async_copy(tokens, own, sems.at[7]),
        pltpu.make_async_copy(gain, gain_out, sems.at[8]),
    ]
    copies += [
        pltpu.make_async_copy(w.at[at, :], held.at[n], sems.at[n]) for n, w in enumerate(weights)
    ]
    for copy in copies:
        copy.start()
    copies[0].wait()
    copies[1].wait()
    values = own[...].astype(F32)
    squares[...] = jnp.broadcast_to(
        jnp.sum(values * values, axis=1, keepdims=True), squares.shape
    )
    piece = (values * gain_out[tags[1]]).astype(BF16)
    for n in range(7):
        copies[2 + n].wait()
        partial[:, n * 256 : (n + 1) * 256] = dot(piece, held[n])


def project(tags, t1, t2, t3, gain, start_squares, extra, started, *refs):
    weights = refs[:7]
    mine, theirs, held, partial, sems = refs[7:]
    here = tags[1]
    core = tags[0]
    rows, width = t1.shape
    blocks = [(here + 4 - s) % 4 for s in (1, 2, 3)]
    copies = [
        [
            pltpu.make_async_copy(
                w.at[pl.ds(pl.multiple_of(block * width, width), width), :],
                held.at[n, s],
                sems.at[n * 3 + s],
            )
            for s, block in enumerate(blocks)
        ]
        for n, w in enumerate(weights)
    ]
    given = pltpu.make_async_copy(started, partial, sems.at[21])
    given.start()
    for group in copies:
        for copy in group:
            copy.start()
    squares = start_squares[:, :1]
    pieces = []
    for tok, block in zip((t1, t2, t3), blocks):
        values = tok[...].astype(F32)
        squares = squares + jnp.sum(values * values, axis=1, keepdims=True)
        pieces.append((values * gain[block]).astype(BF16))
    inv = lax.rsqrt(squares / (4 * width) + EPSILON)
    given.wait()
    for n, group in enumerate(copies):
        total = partial[:, n * 256 : (n + 1) * 256]
        for s, copy in enumerate(group):
            copy.wait()
            total = total + dot(pieces[s], held[n, s])
        total = (total * inv).astype(BF16)
        at = slice(n * 128, (n + 1) * 128)
        first = total[:, :128]
        second = total[:, 128:]
        mine[:, at] = jnp.where(core == 0, first, second)
        theirs[:rows, at] = jnp.where(core == 0, second, first)
    line = jnp.concatenate([extra[...], jnp.zeros((4, 128), F32)], axis=0)
    high = line.astype(BF16).astype(F32)
    middle = (line - high).astype(BF16).astype(F32)
    low = line - high - middle
    theirs[rows:, :] = jnp.zeros((16, theirs.shape[1]), BF16)
    for n, piece in enumerate((high, middle, low)):
        both = jnp.concatenate([piece, jnp.zeros((8, 128), F32)], axis=0)
        theirs[rows:, n * 128 : (n + 1) * 128] = both.astype(BF16)


def join(tags, mine, got, kv, query):
    core = tags[0]
    rows = mine.shape[0]
    for ref, place in ((mine, core), (got, 1 - core)):
        at = pl.ds(pl.multiple_of(place * rows, rows), rows)
        kv[at, :] = ref[:rows, :256]
        query[at, :] = ref[:rows, 256:384]


def pair_up(first, second, both):
    rows = first.shape[0]
    both[:rows] = first[...]
    both[rows:] = second[...]


def triangle_sum(ones, value):
    high = value.astype(BF16)
    rest = value - high.astype(F32)
    middle = rest.astype(BF16)
    low = (rest - middle.astype(F32)).astype(BF16)
    return dot(ones, high) + dot(ones, middle) + dot(ones, low)


def recurrence_local(tags, mine, got, gap, extra, kept, send):
    core = tags[0]
    rows = mine.shape[0]
    sent = got[rows:, :384].astype(F32)
    far = sent[:8, :128] + sent[:8, 128:256] + sent[:8, 256:]
    row = lax.broadcasted_iota(jnp.int32, (rows, rows), 0)
    col = lax.broadcasted_iota(jnp.int32, (rows, rows), 1)
    sub = lax.broadcasted_iota(jnp.int32, (8, HG_KEY), 0)
    a = mine[:, 384:]
    b = got[:rows, 384:]
    blocks = (jnp.where(core == 0, a, b), jnp.where(core == 0, b, a))
    values = [x[:, :128] for x in blocks]
    rec_q = []
    for x in blocks:
        rq = x[:, 128:256].astype(F32)
        rec_q.append(rq / (1.0 + jnp.exp(-rq)) * HG_KEY**-0.5)
    out = [None, None]
    pieces = HG_KEY // 8
    for d in range(2):
        keep = (row >= col) if d == 0 else (row <= col)
        ones = keep.astype(BF16)
        pair = gap[d : d + 1, :]
        share = jnp.where(core == 0, pair[:, :128], pair[:, 128:])
        order = (0, 1) if d == 0 else (1, 0)
        state = None
        before = None
        for n in order:
            forget = blocks[n][:, (2 + d) * 128 : (3 + d) * 128].astype(F32)
            key = share / (1.0 + jnp.exp(forget))
            mine_line = extra[d * 2 : d * 2 + 1, :]
            got_line = far[d * 2 : d * 2 + 1, :]
            line0 = jnp.where(core == n, mine_line, got_line)
            mine_line = extra[d * 2 + 1 : d * 2 + 2, :]
            got_line = far[d * 2 + 1 : d * 2 + 2, :]
            line1 = jnp.where(core == n, mine_line, got_line)
            line = jnp.where(core == 0, line0, line1)
            more = jnp.sum(jnp.where(keep, line, 0.0), axis=1, keepdims=True)
            total = triangle_sum(ones, jnp.log1p(-key)) + more
            last = rows - 1 if d == 0 else 0
            end = total[last : last + 1, :]
            middle = total[rows // 2 : rows // 2 + 1, :]
            near_q = (rec_q[n] * jnp.exp(total - middle)).astype(BF16)
            near_k = (key * jnp.exp(middle - total)).astype(BF16)
            score = jnp.where(keep, dot_nt(near_q, near_k), 0.0).astype(BF16)
            result = dot(score, values[n])
            far_k = (key * jnp.exp(end - total)).astype(BF16)
            piece = dot_tn(values[n], far_k)
            if state is None:
                state = piece
                before = end
                reach = total
            else:
                near = (rec_q[n] * jnp.exp(total)).astype(BF16)
                result = result + dot_nt(near, state.astype(BF16))
                state = jnp.exp(end) * state + piece
                reach = total + before
                before = before + end
            kept[n * rows : (n + 1) * rows, (1 + d) * 128 : (2 + d) * 128] = rec_q[n] * jnp.exp(
                reach
            )
            out[n] = result if out[n] is None else out[n] + result
        high = before.astype(BF16).astype(F32)
        low = before - high
        tail = jnp.where(sub == 0, high, jnp.where(sub == 1, low, 0.0))
        tail = jnp.broadcast_to(tail[None], (pieces, 8, HG_KEY))
        both = jnp.concatenate([state.reshape(pieces, 8, HG_KEY), tail], axis=1)
        send[d * pieces : (d + 1) * pieces] = both.astype(BF16)
    for n in range(2):
        kept[n * rows : (n + 1) * rows, :128] = out[n]


def entering_states(tags, got, init, send, turned):
    me = tags[3]
    peers = got.shape[0]
    pieces = HG_KEY // 8
    which = (me // pieces) * 2 + tags[0]
    turned[...] = init[which].T
    state = turned[pl.ds(pl.multiple_of((me % pieces) * 8, 8), 8), :]
    backward = me >= peers // 2
    for t in range(peers):
        at = jnp.where(backward, peers - 1 - t, t)
        send[at] = state.astype(BF16)
        piece = got[at].astype(F32)
        decay = piece[8:9, :] + piece[9:10, :]
        state = jnp.exp(decay) * state + piece[:8, :]


def absorb(tags, queries, pieces, most_in, sums_in, most_out, sums_out, final):
    rows = queries[0].shape[0]
    lane = lax.broadcasted_iota(jnp.int32, (rows, 128), 1)
    row = lax.broadcasted_iota(jnp.int32, (128, 128), 0)
    diagonal = row == lax.broadcasted_iota(jnp.int32, (128, 128), 1)
    scale = QK_DIM**-0.5 * LOG2E
    key = jnp.concatenate([p[:, :128] for p in pieces], axis=0)
    val = jnp.concatenate([p[:, 128:] for p in pieces], axis=0)
    val = jnp.concatenate([val, jnp.ones(val.shape, BF16)], axis=1)
    for s, query in enumerate(queries):
        none = jnp.zeros_like(query)
        both = jnp.concatenate(
            [jnp.where(lane < QK_DIM, query, none), jnp.where(lane < QK_DIM, none, query)],
            axis=0,
        )
        score = dot_nt(both, key)
        most = jnp.max(score, axis=1, keepdims=True)
        if most_in is not None:
            old = most_in[s][:, :1]
            most = jnp.maximum(most, old)
        weight = jnp.exp2((score - most) * scale).astype(BF16)
        sums = dot(weight, val)
        if most_in is not None:
            sums = sums + jnp.exp2((old - most) * scale) * sums_in[s]
        if final is None:
            most_out[s] = jnp.broadcast_to(most, (2 * rows, 128))
            sums_out[s] = sums
            continue
        target = tags[2] ^ s
        norm = sums[:, 128:]
        final[target, : 2 * rows, :] = (sums[:, :128] / norm).astype(BF16)
        level = most * scale + jnp.log2(norm)
        lines = [
            jnp.sum(jnp.where(diagonal, level[m * 128 : (m + 1) * 128], 0.0), 0, keepdims=True)
            for m in range(2 * rows // 128)
        ]
        line = jnp.concatenate(lines, axis=0)
        high = line.astype(BF16).astype(F32)
        middle = (line - high).astype(BF16).astype(F32)
        low = line - high - middle
        fill = jnp.zeros((4, 128), F32)
        tail = jnp.concatenate([high, middle, low, fill], axis=0)
        final[target, 2 * rows : 2 * rows + 16, :] = tail.astype(BF16)


def four(near, far):
    rows = near.shape[0] // 2
    return near[:rows], near[rows:], far[:rows], far[rows:]


def absorb_first(tags, near, far, *refs):
    most_out, sums_out = refs[-2:]
    absorb(tags, four(near, far), refs[:-2], None, None, most_out, sums_out, None)


def absorb_last(tags, near, far, most_in, sums_in, *refs):
    absorb(tags, four(near, far), refs[:-1], most_in, sums_in, None, None, refs[-1])


def finish_heads(tags, parts, lam, gain_a, kept, states, gain_r, keep, give):
    core = tags[0]
    peers = parts.shape[0]
    row = lax.broadcasted_iota(jnp.int32, (128, 128), 0)
    diagonal = row == lax.broadcasted_iota(jnp.int32, (128, 128), 1)
    results = []
    ending = [states[d * 16 : d * 16 + 16].astype(F32).reshape(HG_KEY, HG_KEY).astype(BF16)
              for d in range(2)]
    for n in range(2):
        ratio = []
        for m in range(2):
            k = m * 2 + n
            levels = []
            for p in range(peers):
                tail = parts[p, 512:528, :].astype(F32)
                line = tail[k : k + 1] + tail[k + 4 : k + 5] + tail[k + 8 : k + 9]
                levels.append(jnp.sum(jnp.where(diagonal, line, 0.0), axis=1, keepdims=True))
            top = functools.reduce(jnp.maximum, levels)
            shares = [jnp.exp2(v - top) for v in levels]
            norm = functools.reduce(jnp.add, shares)
            at = slice(k * 128, (k + 1) * 128)
            both = functools.reduce(
                jnp.add, [w * parts[p, at, :].astype(F32) for p, w in enumerate(shares)]
            )
            ratio.append(both / norm)
        diff = ratio[0] - lam[core] * ratio[1]
        mean = jnp.mean(diff * diff, axis=1, keepdims=True)
        attn = (diff * lax.rsqrt(mean + EPSILON) * gain_a[...]).astype(BF16)
        at = slice(n * 128, (n + 1) * 128)
        total = kept[at, :128]
        for d in range(2):
            reach = kept[at, (1 + d) * 128 : (2 + d) * 128].astype(BF16)
            total = total + dot_nt(reach, ending[d])
        mean = jnp.mean(total * total, axis=1, keepdims=True)
        rec = (total * lax.rsqrt(mean + EPSILON) * gain_r[...]).astype(BF16)
        results.append(jnp.concatenate([attn, rec], axis=1))
    keep[...] = jnp.where(core == 0, results[0], results[1])
    give[...] = jnp.where(core == 0, results[1], results[0])


def project_out(tags, keep, got, wa, wr, mixed):
    core = tags[0]
    own = pl.ds(pl.multiple_of(core * 128, 128), 128)
    other = pl.ds(pl.multiple_of((1 - core) * 128, 128), 128)
    result = dot(keep[:, :128], wa[own, :]) + dot(got[:, :128], wa[other, :])
    result = result + dot(keep[:, 128:], wr[own, :]) + dot(got[:, 128:], wr[other, :])
    pieces = mixed.shape[0]
    mixed[...] = result.astype(BF16).reshape(pieces, result.shape[0] // pieces, result.shape[1])


def add_up(parts, out):
    total = functools.reduce(jnp.add, [parts[p].astype(F32) for p in range(parts.shape[0])])
    out[...] = total.astype(BF16)


def local(
    tokens,
    norm_gain,
    da_query,
    da_key,
    da_value,
    mix_lambda,
    attn_gain,
    rec_query,
    rec_forget_fwd,
    rec_forget_bwd,
    rec_value,
    gate_gap,
    extra_decay,
    init_state,
    rec_gain,
    out_attn,
    out_rec,
):
    rows, width = tokens.shape
    tags = jnp.stack(
        [lax.axis_index(C), lax.axis_index(Y), lax.axis_index(X), lax.axis_index((Z, X))]
    ).astype(jnp.int32)

    extra = jnp.transpose(extra_decay, (0, 2, 1)).reshape(4, rows)
    toks = {s: shifted(tokens, Y, s) for s in (2, 1, 3)}
    weights = [
        da_key,
        da_value,
        da_query,
        rec_value,
        rec_query,
        rec_forget_fwd,
        rec_forget_bwd,
    ]
    partial, gain, squares = call(
        begin,
        [((rows, 7 * 256), F32), ((4, 1, width), F32), ((rows, 128), F32)],
        [tags, tokens, norm_gain.reshape(4, 1, width), *weights],
        scratch=[
            pltpu.VMEM((rows, width), BF16),
            pltpu.VMEM((7, width, 256), BF16),
            pltpu.SemaphoreType.DMA((9,)),
        ],
        specs=[SMEM] + [HBM] * 9,
        flops=2 * rows * width * 7 * 256,
        mib=53,
    )
    mine, theirs = call(
        project,
        [((rows, 7 * 128), BF16), ((rows + 16, 7 * 128), BF16)],
        [tags, toks[1], toks[2], toks[3], gain, squares, extra, partial, *weights],
        scratch=[
            pltpu.VMEM((7, 3, width, 256), BF16),
            pltpu.VMEM((rows, 7 * 256), F32),
            pltpu.SemaphoreType.DMA((22,)),
        ],
        specs=[SMEM] + [VMEM] * 6 + [HBM] * 8,
        flops=2 * rows * D * 7 * 256,
        mib=53,
    )
    got = shifted(theirs, C, 1)
    kv, query = call(
        join,
        [((2 * rows, 256), BF16), ((2 * rows, 128), BF16)],
        [tags, mine, got],
        specs=[SMEM, VMEM, VMEM],
    )

    up = shifted(kv, Z, 1)
    down = shifted(kv, Z, 7)
    kept, send = call(
        recurrence_local,
        [((2 * rows, 3 * 128), F32), ((32, 16, 128), BF16)],
        [tags, mine, got, gate_gap, extra],
        specs=[SMEM] + [VMEM] * 4,
        flops=2 * rows * 128 * 128 * 40,
    )
    arrived = lax.all_to_all(send, (Z, X), 0, 0, tiled=True)
    up2 = shifted(up, Z, 1)
    down2 = shifted(down, Z, 7)
    beside = lax.ppermute(query, X, [(i, i ^ 1) for i in range(4)])
    near = call(pair_up, ((4 * rows, 128), BF16), [query, beside])
    queries = [near, lax.ppermute(near, X, [(i, i ^ 2) for i in range(4)])]
    back = call(
        entering_states,
        ((32, 8, 128), BF16),
        [tags, arrived, init_state.reshape(-1, HG_KEY, HG_KEY)],
        scratch=[pltpu.VMEM((HG_KEY, HG_KEY), F32)],
        specs=[SMEM, VMEM, VMEM],
    )
    up3 = shifted(up2, Z, 1)
    down3 = shifted(down2, Z, 7)
    states = lax.all_to_all(back, (Z, X), 0, 0, tiled=True)
    flops = 4 * 512 * 256 * 2 * 2 * 256
    most, sums = call(
        absorb_first,
        [((4, 4 * rows, 128), F32), ((4, 4 * rows, 256), F32)],
        [tags, *queries, kv, up, down, up2, down2],
        specs=[SMEM] + [VMEM] * 7,
        flops=5 * flops,
        mib=16,
    )
    up4 = shifted(up3, Z, 1)
    parts = call(
        absorb_last,
        ((4, 4 * rows + 16, 128), BF16),
        [tags, *queries, most, sums, up3, down3, up4],
        specs=[SMEM] + [VMEM] * 7,
        flops=3 * flops,
        mib=12,
    )
    parts = lax.all_to_all(parts, X, 0, 0, tiled=True)
    keep, give = call(
        finish_heads,
        [((rows, 256), BF16)] * 2,
        [tags, parts, mix_lambda, attn_gain[None], kept, states, rec_gain[None]],
        specs=[SMEM, VMEM, SMEM] + [VMEM] * 4,
    )
    got = shifted(give, C, 1)
    mixed = call(
        project_out,
        ((4, rows // 4, D), BF16),
        [tags, keep, got, out_attn, out_rec],
        specs=[SMEM] + [VMEM] * 4,
        flops=2 * rows * D * 512,
    )
    mixed = lax.all_to_all(mixed, Y, 0, 0, tiled=True)
    return call(add_up, ((rows // 4, D), BF16), [mixed])


def solution(mesh):
    torus = Mesh(mesh.devices.reshape(8, 4, 2, mesh.shape["tp"]), (Z, X, C, Y))
    return jax.shard_map(
        local,
        mesh=torus,
        in_specs=(
            P(SP, Y),
            P(),
            P(None, Y),
            P(None, Y),
            P(None, Y),
            P(Y),
            P(),
            P(None, Y),
            P(None, Y),
            P(None, Y),
            P(None, Y),
            P(None, Y),
            P(None, SP, Y),
            P(None, Y, None, None),
            P(),
            P(Y, None),
            P(Y, None),
        ),
        out_specs=P((*SP, Y), None),
        check_vma=False,
    )
```

```python
import functools

import jax
import jax.numpy as jnp
from jax import lax
from jax.experimental import pallas as pl
from jax.experimental.pallas import tpu as pltpu
from jax.sharding import Mesh
from jax.sharding import PartitionSpec as P

D = 2048
QK_DIM = 64
HG_KEY = 128
EPSILON = 1e-06
LOG2E = 1.4426950408889634
Z, X, C, Y = ("z", "x", "c", "y")
SP = (Z, X, C)
F32 = jnp.float32
BF16 = jnp.bfloat16


VMEM = pl.BlockSpec(memory_space=pltpu.VMEM)
SMEM = pl.BlockSpec(memory_space=pltpu.SMEM)
HBM = pl.BlockSpec(memory_space=pltpu.HBM)


def call(body, out, ins, scratch=(), specs=None, flops=0, mib=4):
    one = isinstance(out, tuple)
    outs = [out] if one else list(out)
    shapes = [jax.ShapeDtypeStruct(s, t) for s, t in outs]
    specs = specs or [VMEM] * len(ins)
    done = pl.pallas_call(
        body,
        out_shape=shapes,
        in_specs=specs,
        out_specs=[VMEM] * len(shapes),
        scratch_shapes=list(scratch),
        cost_estimate=pl.CostEstimate(flops=flops, transcendentals=0, bytes_accessed=0),
        compiler_params=pltpu.CompilerParams(vmem_limit_bytes=mib << 20),
    )(*ins)
    return done[0] if one else done


def dot(a, b):
    return lax.dot_general(a, b, (((1,), (0,)), ((), ())), preferred_element_type=F32)


def dot_nt(a, b):
    return lax.dot_general(a, b, (((1,), (1,)), ((), ())), preferred_element_type=F32)


def dot_tn(a, b):
    return lax.dot_general(a, b, (((0,), (0,)), ((), ())), preferred_element_type=F32)


def shifted(value, axis, by):
    peers = lax.axis_size(axis)
    return lax.ppermute(value, axis, [(i, (i + by) % peers) for i in range(peers)])


def begin(tags, tokens, gain, *refs):
    weights = refs[:7]
    partial, gain_out, squares, own, held, sems = refs[7:]
    width = tokens.shape[1]
    at = pl.ds(pl.multiple_of(tags[1] * width, width), width)
    copies = [
        pltpu.make_async_copy(tokens, own, sems.at[7]),
        pltpu.make_async_copy(gain, gain_out, sems.at[8]),
    ]
    copies += [
        pltpu.make_async_copy(w.at[at, :], held.at[n], sems.at[n]) for n, w in enumerate(weights)
    ]
    for copy in copies:
        copy.start()
    for copy in copies:
        copy.wait()
    values = own[...].astype(F32)
    squares[...] = jnp.broadcast_to(
        jnp.sum(values * values, axis=1, keepdims=True), squares.shape
    )
    piece = (values * gain_out[tags[1]]).astype(BF16)
    for n in range(7):
        partial[:, n * 256 : (n + 1) * 256] = dot(piece, held[n])


def project(tags, t1, t2, t3, gain, start_squares, extra, started, *refs):
    weights = refs[:7]
    mine, theirs, held, partial, sems = refs[7:]
    here = tags[1]
    core = tags[0]
    rows, width = t1.shape
    blocks = [(here + 4 - s) % 4 for s in (1, 2, 3)]
    copies = [
        [
            pltpu.make_async_copy(
                w.at[pl.ds(pl.multiple_of(block * width, width), width), :],
                held.at[n, pl.ds(s * width, width), :],
                sems.at[n * 3 + s],
            )
            for s, block in enumerate(blocks)
        ]
        for n, w in enumerate(weights)
    ]
    given = pltpu.make_async_copy(started, partial, sems.at[21])
    given.start()
    for group in copies:
        for copy in group:
            copy.start()
    squares = start_squares[:, :1]
    pieces = []
    for tok, block in zip((t1, t2, t3), blocks):
        values = tok[...].astype(F32)
        squares = squares + jnp.sum(values * values, axis=1, keepdims=True)
        pieces.append((values * gain[block]).astype(BF16))
    inv = lax.rsqrt(squares / (4 * width) + EPSILON)
    given.wait()
    for group in copies:
        for copy in group:
            copy.wait()
    joined = jnp.concatenate(pieces, axis=1)
    for n in range(7):
        total = partial[:, n * 256 : (n + 1) * 256] + dot(joined, held[n])
        total = (total * inv).astype(BF16)
        at = slice(n * 128, (n + 1) * 128)
        first = total[:, :128]
        second = total[:, 128:]
        mine[:, at] = jnp.where(core == 0, first, second)
        theirs[:rows, at] = jnp.where(core == 0, second, first)
    line = jnp.concatenate([extra[...], jnp.zeros((4, 128), F32)], axis=0)
    high = line.astype(BF16).astype(F32)
    middle = (line - high).astype(BF16).astype(F32)
    low = line - high - middle
    theirs[rows:, :] = jnp.zeros((16, theirs.shape[1]), BF16)
    for n, piece in enumerate((high, middle, low)):
        both = jnp.concatenate([piece, jnp.zeros((8, 128), F32)], axis=0)
        theirs[rows:, n * 128 : (n + 1) * 128] = both.astype(BF16)


def join(tags, mine, got, kv, query):
    core = tags[0]
    rows = mine.shape[0]
    for ref, place in ((mine, core), (got, 1 - core)):
        at = pl.ds(pl.multiple_of(place * rows, rows), rows)
        kv[at, :] = ref[:rows, :256]
        query[at, :] = ref[:rows, 256:384]


def pair_up(first, second, both):
    rows = first.shape[0]
    both[:rows] = first[...]
    both[rows:] = second[...]


def triangle_sum(ones, value):
    high = value.astype(BF16)
    rest = value - high.astype(F32)
    middle = rest.astype(BF16)
    low = (rest - middle.astype(F32)).astype(BF16)
    return dot(ones, high) + dot(ones, middle) + dot(ones, low)


def recurrence_local(tags, mine, got, gap, extra, kept, send):
    core = tags[0]
    rows = mine.shape[0]
    sent = got[rows:, :384].astype(F32)
    far = sent[:8, :128] + sent[:8, 128:256] + sent[:8, 256:]
    row = lax.broadcasted_iota(jnp.int32, (rows, rows), 0)
    col = lax.broadcasted_iota(jnp.int32, (rows, rows), 1)
    sub = lax.broadcasted_iota(jnp.int32, (8, HG_KEY), 0)
    a = mine[:, 384:]
    b = got[:rows, 384:]
    blocks = (jnp.where(core == 0, a, b), jnp.where(core == 0, b, a))
    values = [x[:, :128] for x in blocks]
    rec_q = []
    for x in blocks:
        rq = x[:, 128:256].astype(F32)
        rec_q.append(rq / (1.0 + jnp.exp(-rq)) * HG_KEY**-0.5)
    out = [None, None]
    pieces = HG_KEY // 8
    for d in range(2):
        keep = (row >= col) if d == 0 else (row <= col)
        ones = keep.astype(BF16)
        pair = gap[d : d + 1, :]
        share = jnp.where(core == 0, pair[:, :128], pair[:, 128:])
        order = (0, 1) if d == 0 else (1, 0)
        state = None
        before = None
        for n in order:
            forget = blocks[n][:, (2 + d) * 128 : (3 + d) * 128].astype(F32)
            key = share / (1.0 + jnp.exp(forget))
            mine_line = extra[d * 2 : d * 2 + 1, :]
            got_line = far[d * 2 : d * 2 + 1, :]
            line0 = jnp.where(core == n, mine_line, got_line)
            mine_line = extra[d * 2 + 1 : d * 2 + 2, :]
            got_line = far[d * 2 + 1 : d * 2 + 2, :]
            line1 = jnp.where(core == n, mine_line, got_line)
            line = jnp.where(core == 0, line0, line1)
            more = jnp.sum(jnp.where(keep, line, 0.0), axis=1, keepdims=True)
            total = triangle_sum(ones, jnp.log1p(-key)) + more
            last = rows - 1 if d == 0 else 0
            end = total[last : last + 1, :]
            middle = total[rows // 2 : rows // 2 + 1, :]
            near_q = (rec_q[n] * jnp.exp(total - middle)).astype(BF16)
            near_k = (key * jnp.exp(middle - total)).astype(BF16)
            score = jnp.where(keep, dot_nt(near_q, near_k), 0.0).astype(BF16)
            result = dot(score, values[n])
            far_k = (key * jnp.exp(end - total)).astype(BF16)
            piece = dot_tn(values[n], far_k)
            if state is None:
                state = piece
                before = end
                reach = total
            else:
                near = (rec_q[n] * jnp.exp(total)).astype(BF16)
                result = result + dot_nt(near, state.astype(BF16))
                state = jnp.exp(end) * state + piece
                reach = total + before
                before = before + end
            kept[n * rows : (n + 1) * rows, (1 + d) * 128 : (2 + d) * 128] = rec_q[n] * jnp.exp(
                reach
            )
            out[n] = result if out[n] is None else out[n] + result
        high = before.astype(BF16).astype(F32)
        low = before - high
        tail = jnp.where(sub == 0, high, jnp.where(sub == 1, low, 0.0))
        tail = jnp.broadcast_to(tail[None], (pieces, 8, HG_KEY))
        both = jnp.concatenate([state.reshape(pieces, 8, HG_KEY), tail], axis=1)
        send[d * pieces : (d + 1) * pieces] = both.astype(BF16)
    for n in range(2):
        kept[n * rows : (n + 1) * rows, :128] = out[n]


def entering_states(tags, got, init, send, turned):
    me = tags[3]
    peers = got.shape[0]
    pieces = HG_KEY // 8
    which = (me // pieces) * 2 + tags[0]
    turned[...] = init[which].T
    state = turned[pl.ds(pl.multiple_of((me % pieces) * 8, 8), 8), :]
    backward = me >= peers // 2
    for t in range(peers):
        at = jnp.where(backward, peers - 1 - t, t)
        send[at] = state.astype(BF16)
        piece = got[at].astype(F32)
        decay = piece[8:9, :] + piece[9:10, :]
        state = jnp.exp(decay) * state + piece[:8, :]


def absorb(tags, queries, pieces, most_in, sums_in, most_out, sums_out, final):
    rows = queries[0].shape[0]
    lane = lax.broadcasted_iota(jnp.int32, (rows, 128), 1)
    row = lax.broadcasted_iota(jnp.int32, (128, 128), 0)
    diagonal = row == lax.broadcasted_iota(jnp.int32, (128, 128), 1)
    scale = QK_DIM**-0.5 * LOG2E
    key = jnp.concatenate([p[:, :128] for p in pieces], axis=0)
    val = jnp.concatenate([p[:, 128:] for p in pieces], axis=0)
    val = jnp.concatenate([val, jnp.ones(val.shape, BF16)], axis=1)
    for s, query in enumerate(queries):
        none = jnp.zeros_like(query)
        both = jnp.concatenate(
            [jnp.where(lane < QK_DIM, query, none), jnp.where(lane < QK_DIM, none, query)],
            axis=0,
        )
        score = dot_nt(both, key)
        most = jnp.max(score, axis=1, keepdims=True)
        if most_in is not None:
            old = most_in[s][:, :1]
            most = jnp.maximum(most, old)
        weight = jnp.exp2((score - most) * scale).astype(BF16)
        sums = dot(weight, val)
        if most_in is not None:
            sums = sums + jnp.exp2((old - most) * scale) * sums_in[s]
        if final is None:
            most_out[s] = jnp.broadcast_to(most, (2 * rows, 128))
            sums_out[s] = sums
            continue
        target = tags[2] ^ s
        norm = sums[:, 128:]
        final[target, : 2 * rows, :] = (sums[:, :128] / norm).astype(BF16)
        level = most * scale + jnp.log2(norm)
        lines = [
            jnp.sum(jnp.where(diagonal, level[m * 128 : (m + 1) * 128], 0.0), 0, keepdims=True)
            for m in range(2 * rows // 128)
        ]
        line = jnp.concatenate(lines, axis=0)
        high = line.astype(BF16).astype(F32)
        middle = (line - high).astype(BF16).astype(F32)
        low = line - high - middle
        fill = jnp.zeros((4, 128), F32)
        tail = jnp.concatenate([high, middle, low, fill], axis=0)
        final[target, 2 * rows : 2 * rows + 16, :] = tail.astype(BF16)


def four(near, far):
    rows = near.shape[0] // 2
    return near[:rows], near[rows:], far[:rows], far[rows:]


def absorb_first(tags, near, far, *refs):
    most_out, sums_out = refs[-2:]
    absorb(tags, four(near, far), refs[:-2], None, None, most_out, sums_out, None)


def absorb_last(tags, near, far, most_in, sums_in, *refs):
    absorb(tags, four(near, far), refs[:-1], most_in, sums_in, None, None, refs[-1])


def finish_heads(tags, parts, lam, gain_a, kept, states, gain_r, keep, give):
    core = tags[0]
    peers = parts.shape[0]
    row = lax.broadcasted_iota(jnp.int32, (128, 128), 0)
    diagonal = row == lax.broadcasted_iota(jnp.int32, (128, 128), 1)
    results = []
    ending = [states[d * 16 : d * 16 + 16].astype(F32).reshape(HG_KEY, HG_KEY).astype(BF16)
              for d in range(2)]
    for n in range(2):
        ratio = []
        for m in range(2):
            k = m * 2 + n
            levels = []
            for p in range(peers):
                tail = parts[p, 512:528, :].astype(F32)
                line = tail[k : k + 1] + tail[k + 4 : k + 5] + tail[k + 8 : k + 9]
                levels.append(jnp.sum(jnp.where(diagonal, line, 0.0), axis=1, keepdims=True))
            top = functools.reduce(jnp.maximum, levels)
            shares = [jnp.exp2(v - top) for v in levels]
            norm = functools.reduce(jnp.add, shares)
            at = slice(k * 128, (k + 1) * 128)
            both = functools.reduce(
                jnp.add, [w * parts[p, at, :].astype(F32) for p, w in enumerate(shares)]
            )
            ratio.append(both / norm)
        diff = ratio[0] - lam[core] * ratio[1]
        mean = jnp.mean(diff * diff, axis=1, keepdims=True)
        attn = (diff * lax.rsqrt(mean + EPSILON) * gain_a[...]).astype(BF16)
        at = slice(n * 128, (n + 1) * 128)
        total = kept[at, :128]
        for d in range(2):
            reach = kept[at, (1 + d) * 128 : (2 + d) * 128].astype(BF16)
            total = total + dot_nt(reach, ending[d])
        mean = jnp.mean(total * total, axis=1, keepdims=True)
        rec = (total * lax.rsqrt(mean + EPSILON) * gain_r[...]).astype(BF16)
        results.append(jnp.concatenate([attn, rec], axis=1))
    keep[...] = jnp.where(core == 0, results[0], results[1])
    give[...] = jnp.where(core == 0, results[1], results[0])


def project_out(tags, keep, got, wa, wr, mixed):
    core = tags[0]
    own = pl.ds(pl.multiple_of(core * 128, 128), 128)
    other = pl.ds(pl.multiple_of((1 - core) * 128, 128), 128)
    result = dot(keep[:, :128], wa[own, :]) + dot(got[:, :128], wa[other, :])
    result = result + dot(keep[:, 128:], wr[own, :]) + dot(got[:, 128:], wr[other, :])
    pieces = mixed.shape[0]
    mixed[...] = result.astype(BF16).reshape(pieces, result.shape[0] // pieces, result.shape[1])


def add_up(parts, out):
    total = functools.reduce(jnp.add, [parts[p].astype(F32) for p in range(parts.shape[0])])
    out[...] = total.astype(BF16)


def local(
    tokens,
    norm_gain,
    da_query,
    da_key,
    da_value,
    mix_lambda,
    attn_gain,
    rec_query,
    rec_forget_fwd,
    rec_forget_bwd,
    rec_value,
    gate_gap,
    extra_decay,
    init_state,
    rec_gain,
    out_attn,
    out_rec,
):
    rows, width = tokens.shape
    tags = jnp.stack(
        [lax.axis_index(C), lax.axis_index(Y), lax.axis_index(X), lax.axis_index((Z, X))]
    ).astype(jnp.int32)

    extra = jnp.transpose(extra_decay, (0, 2, 1)).reshape(4, rows)
    toks = {s: shifted(tokens, Y, s) for s in (2, 1, 3)}
    weights = [
        da_key,
        da_value,
        da_query,
        rec_value,
        rec_query,
        rec_forget_fwd,
        rec_forget_bwd,
    ]
    partial, gain, squares = call(
        begin,
        [((rows, 7 * 256), F32), ((4, 1, width), F32), ((rows, 128), F32)],
        [tags, tokens, norm_gain.reshape(4, 1, width), *weights],
        scratch=[
            pltpu.VMEM((rows, width), BF16),
            pltpu.VMEM((7, width, 256), BF16),
            pltpu.SemaphoreType.DMA((9,)),
        ],
        specs=[SMEM] + [HBM] * 9,
        flops=2 * rows * width * 7 * 256,
        mib=53,
    )
    mine, theirs = call(
        project,
        [((rows, 7 * 128), BF16), ((rows + 16, 7 * 128), BF16)],
        [tags, toks[1], toks[2], toks[3], gain, squares, extra, partial, *weights],
        scratch=[
            pltpu.VMEM((7, 3 * width, 256), BF16),
            pltpu.VMEM((rows, 7 * 256), F32),
            pltpu.SemaphoreType.DMA((22,)),
        ],
        specs=[SMEM] + [VMEM] * 6 + [HBM] * 8,
        flops=2 * rows * D * 7 * 256,
        mib=53,
    )
    got = shifted(theirs, C, 1)
    kv, query = call(
        join,
        [((2 * rows, 256), BF16), ((2 * rows, 128), BF16)],
        [tags, mine, got],
        specs=[SMEM, VMEM, VMEM],
    )

    up = shifted(kv, Z, 1)
    down = shifted(kv, Z, 7)
    kept, send = call(
        recurrence_local,
        [((2 * rows, 3 * 128), F32), ((32, 16, 128), BF16)],
        [tags, mine, got, gate_gap, extra],
        specs=[SMEM] + [VMEM] * 4,
        flops=2 * rows * 128 * 128 * 40,
    )
    arrived = lax.all_to_all(send, (Z, X), 0, 0, tiled=True)
    up2 = shifted(up, Z, 1)
    down2 = shifted(down, Z, 7)
    beside = lax.ppermute(query, X, [(i, i ^ 1) for i in range(4)])
    near = call(pair_up, ((4 * rows, 128), BF16), [query, beside])
    queries = [near, lax.ppermute(near, X, [(i, i ^ 2) for i in range(4)])]
    back = call(
        entering_states,
        ((32, 8, 128), BF16),
        [tags, arrived, init_state.reshape(-1, HG_KEY, HG_KEY)],
        scratch=[pltpu.VMEM((HG_KEY, HG_KEY), F32)],
        specs=[SMEM, VMEM, VMEM],
    )
    up3 = shifted(up2, Z, 1)
    down3 = shifted(down2, Z, 7)
    states = lax.all_to_all(back, (Z, X), 0, 0, tiled=True)
    flops = 4 * 512 * 256 * 2 * 2 * 256
    most, sums = call(
        absorb_first,
        [((4, 4 * rows, 128), F32), ((4, 4 * rows, 256), F32)],
        [tags, *queries, kv, up, down, up2, down2],
        specs=[SMEM] + [VMEM] * 7,
        flops=5 * flops,
        mib=16,
    )
    up4 = shifted(up3, Z, 1)
    parts = call(
        absorb_last,
        ((4, 4 * rows + 16, 128), BF16),
        [tags, *queries, most, sums, up3, down3, up4],
        specs=[SMEM] + [VMEM] * 7,
        flops=3 * flops,
        mib=12,
    )
    parts = lax.all_to_all(parts, X, 0, 0, tiled=True)
    keep, give = call(
        finish_heads,
        [((rows, 256), BF16)] * 2,
        [tags, parts, mix_lambda, attn_gain[None], kept, states, rec_gain[None]],
        specs=[SMEM, VMEM, SMEM] + [VMEM] * 4,
    )
    got = shifted(give, C, 1)
    mixed = call(
        project_out,
        ((4, rows // 4, D), BF16),
        [tags, keep, got, out_attn, out_rec],
        specs=[SMEM] + [VMEM] * 4,
        flops=2 * rows * D * 512,
    )
    mixed = lax.all_to_all(mixed, Y, 0, 0, tiled=True)
    return call(add_up, ((rows // 4, D), BF16), [mixed])


def solution(mesh):
    torus = Mesh(mesh.devices.reshape(8, 4, 2, mesh.shape["tp"]), (Z, X, C, Y))
    return jax.shard_map(
        local,
        mesh=torus,
        in_specs=(
            P(SP, Y),
            P(),
            P(None, Y),
            P(None, Y),
            P(None, Y),
            P(Y),
            P(),
            P(None, Y),
            P(None, Y),
            P(None, Y),
            P(None, Y),
            P(None, Y),
            P(None, SP, Y),
            P(None, Y, None, None),
            P(),
            P(Y, None),
            P(Y, None),
        ),
        out_specs=P((*SP, Y), None),
        check_vma=False,
    )
```

```python
import functools

import jax
import jax.numpy as jnp
from jax import lax
from jax.experimental import pallas as pl
from jax.experimental.pallas import tpu as pltpu
from jax.sharding import Mesh
from jax.sharding import PartitionSpec as P

D = 2048
QK_DIM = 64
HG_KEY = 128
EPSILON = 1e-06
LOG2E = 1.4426950408889634
Z, X, C, Y = ("z", "x", "c", "y")
SP = (Z, X, C)
F32 = jnp.float32
BF16 = jnp.bfloat16


VMEM = pl.BlockSpec(memory_space=pltpu.VMEM)
SMEM = pl.BlockSpec(memory_space=pltpu.SMEM)
HBM = pl.BlockSpec(memory_space=pltpu.HBM)


def call(body, out, ins, scratch=(), specs=None, flops=0, mib=4):
    one = isinstance(out, tuple)
    outs = [out] if one else list(out)
    shapes = [jax.ShapeDtypeStruct(s, t) for s, t in outs]
    specs = specs or [VMEM] * len(ins)
    done = pl.pallas_call(
        body,
        out_shape=shapes,
        in_specs=specs,
        out_specs=[VMEM] * len(shapes),
        scratch_shapes=list(scratch),
        cost_estimate=pl.CostEstimate(flops=flops, transcendentals=0, bytes_accessed=0),
        compiler_params=pltpu.CompilerParams(vmem_limit_bytes=mib << 20),
    )(*ins)
    return done[0] if one else done


def dot(a, b):
    return lax.dot_general(a, b, (((1,), (0,)), ((), ())), preferred_element_type=F32)


def dot_nt(a, b):
    return lax.dot_general(a, b, (((1,), (1,)), ((), ())), preferred_element_type=F32)


def dot_tn(a, b):
    return lax.dot_general(a, b, (((0,), (0,)), ((), ())), preferred_element_type=F32)


def swapped(value, axis, by):
    return lax.ppermute(value, axis, [(i, i ^ by) for i in range(lax.axis_size(axis))])


def shifted(value, axis, by):
    peers = lax.axis_size(axis)
    return lax.ppermute(value, axis, [(i, (i + by) % peers) for i in range(peers)])


def begin(tags, tokens, gain, *refs):
    weights = refs[:7]
    partial, gain_out, squares, own, held, sems = refs[7:]
    width = tokens.shape[1]
    at = pl.ds(pl.multiple_of(tags[1] * width, width), width)
    copies = [
        pltpu.make_async_copy(tokens, own, sems.at[7]),
        pltpu.make_async_copy(gain, gain_out, sems.at[8]),
    ]
    copies += [
        pltpu.make_async_copy(w.at[at, :], held.at[n], sems.at[n]) for n, w in enumerate(weights)
    ]
    for copy in copies:
        copy.start()
    for copy in copies:
        copy.wait()
    values = own[...].astype(F32)
    squares[...] = jnp.broadcast_to(
        jnp.sum(values * values, axis=1, keepdims=True), squares.shape
    )
    piece = (values * gain_out[tags[1]]).astype(BF16)
    for n in range(7):
        partial[:, n * 256 : (n + 1) * 256] = dot(piece, held[n])


def project(tags, t1, t2, t3, gain, start_squares, extra, started, *refs):
    weights = refs[:7]
    mine, theirs, held, partial, sems = refs[7:]
    here = tags[1]
    core = tags[0]
    rows, width = t1.shape
    blocks = [(here + 4 - s) % 4 for s in (1, 2, 3)]
    copies = [
        [
            pltpu.make_async_copy(
                w.at[pl.ds(pl.multiple_of(block * width, width), width), :],
                held.at[n, pl.ds(s * width, width), :],
                sems.at[n * 3 + s],
            )
            for s, block in enumerate(blocks)
        ]
        for n, w in enumerate(weights)
    ]
    given = pltpu.make_async_copy(started, partial, sems.at[21])
    given.start()
    for group in copies:
        for copy in group:
            copy.start()
    squares = start_squares[:, :1]
    pieces = []
    for tok, block in zip((t1, t2, t3), blocks):
        values = tok[...].astype(F32)
        squares = squares + jnp.sum(values * values, axis=1, keepdims=True)
        pieces.append((values * gain[block]).astype(BF16))
    inv = lax.rsqrt(squares / (4 * width) + EPSILON)
    given.wait()
    for group in copies:
        for copy in group:
            copy.wait()
    joined = jnp.concatenate(pieces, axis=1)
    for n in range(7):
        total = partial[:, n * 256 : (n + 1) * 256] + dot(joined, held[n])
        total = (total * inv).astype(BF16)
        at = slice(n * 128, (n + 1) * 128)
        first = total[:, :128]
        second = total[:, 128:]
        mine[:, at] = jnp.where(core == 0, first, second)
        theirs[:rows, at] = jnp.where(core == 0, second, first)
    line = jnp.concatenate([extra[...], jnp.zeros((4, 128), F32)], axis=0)
    high = line.astype(BF16).astype(F32)
    middle = (line - high).astype(BF16).astype(F32)
    low = line - high - middle
    theirs[rows:, :] = jnp.zeros((16, theirs.shape[1]), BF16)
    for n, piece in enumerate((high, middle, low)):
        both = jnp.concatenate([piece, jnp.zeros((8, 128), F32)], axis=0)
        theirs[rows:, n * 128 : (n + 1) * 128] = both.astype(BF16)


def join(tags, mine, got, kv, query):
    core = tags[0]
    rows = mine.shape[0]
    for ref, place in ((mine, core), (got, 1 - core)):
        at = pl.ds(pl.multiple_of(place * rows, rows), rows)
        kv[at, :] = ref[:rows, :256]
        query[at, :] = ref[:rows, 256:384]


def pair_up(first, second, both):
    rows = first.shape[0]
    both[:rows] = first[...]
    both[rows:] = second[...]


def triangle_sum(ones, value):
    high = value.astype(BF16)
    rest = value - high.astype(F32)
    middle = rest.astype(BF16)
    low = (rest - middle.astype(F32)).astype(BF16)
    return dot(ones, high) + dot(ones, middle) + dot(ones, low)


def recurrence_local(tags, mine, got, gap, extra, kept, send):
    core = tags[0]
    rows = mine.shape[0]
    sent = got[rows:, :384].astype(F32)
    far = sent[:8, :128] + sent[:8, 128:256] + sent[:8, 256:]
    row = lax.broadcasted_iota(jnp.int32, (rows, rows), 0)
    col = lax.broadcasted_iota(jnp.int32, (rows, rows), 1)
    sub = lax.broadcasted_iota(jnp.int32, (8, HG_KEY), 0)
    a = mine[:, 384:]
    b = got[:rows, 384:]
    blocks = (jnp.where(core == 0, a, b), jnp.where(core == 0, b, a))
    values = [x[:, :128] for x in blocks]
    rec_q = []
    for x in blocks:
        rq = x[:, 128:256].astype(F32)
        rec_q.append(rq / (1.0 + jnp.exp(-rq)) * HG_KEY**-0.5)
    out = [None, None]
    pieces = HG_KEY // 8
    for d in range(2):
        keep = (row >= col) if d == 0 else (row <= col)
        ones = keep.astype(BF16)
        pair = gap[d : d + 1, :]
        share = jnp.where(core == 0, pair[:, :128], pair[:, 128:])
        order = (0, 1) if d == 0 else (1, 0)
        state = None
        before = None
        for n in order:
            forget = blocks[n][:, (2 + d) * 128 : (3 + d) * 128].astype(F32)
            key = share / (1.0 + jnp.exp(forget))
            mine_line = extra[d * 2 : d * 2 + 1, :]
            got_line = far[d * 2 : d * 2 + 1, :]
            line0 = jnp.where(core == n, mine_line, got_line)
            mine_line = extra[d * 2 + 1 : d * 2 + 2, :]
            got_line = far[d * 2 + 1 : d * 2 + 2, :]
            line1 = jnp.where(core == n, mine_line, got_line)
            line = jnp.where(core == 0, line0, line1)
            more = jnp.sum(jnp.where(keep, line, 0.0), axis=1, keepdims=True)
            total = triangle_sum(ones, jnp.log1p(-key)) + more
            last = rows - 1 if d == 0 else 0
            end = total[last : last + 1, :]
            middle = total[rows // 2 : rows // 2 + 1, :]
            near_q = (rec_q[n] * jnp.exp(total - middle)).astype(BF16)
            near_k = (key * jnp.exp(middle - total)).astype(BF16)
            score = jnp.where(keep, dot_nt(near_q, near_k), 0.0).astype(BF16)
            result = dot(score, values[n])
            far_k = (key * jnp.exp(end - total)).astype(BF16)
            piece = dot_tn(values[n], far_k)
            if state is None:
                state = piece
                before = end
                reach = total
            else:
                near = (rec_q[n] * jnp.exp(total)).astype(BF16)
                result = result + dot_nt(near, state.astype(BF16))
                state = jnp.exp(end) * state + piece
                reach = total + before
                before = before + end
            kept[n * rows : (n + 1) * rows, (1 + d) * 128 : (2 + d) * 128] = rec_q[n] * jnp.exp(
                reach
            )
            out[n] = result if out[n] is None else out[n] + result
        high = before.astype(BF16).astype(F32)
        low = before - high
        tail = jnp.where(sub == 0, high, jnp.where(sub == 1, low, 0.0))
        tail = jnp.broadcast_to(tail[None], (pieces, 8, HG_KEY))
        both = jnp.concatenate([state.reshape(pieces, 8, HG_KEY), tail], axis=1)
        send[d * pieces : (d + 1) * pieces] = both.astype(BF16)
    for n in range(2):
        kept[n * rows : (n + 1) * rows, :128] = out[n]


def entering_states(tags, got, init, send, turned):
    me = tags[3]
    peers = got.shape[0]
    pieces = HG_KEY // 8
    which = (me // pieces) * 2 + tags[0]
    turned[...] = init[which].T
    state = turned[pl.ds(pl.multiple_of((me % pieces) * 8, 8), 8), :]
    backward = me >= peers // 2
    for t in range(peers):
        at = jnp.where(backward, peers - 1 - t, t)
        send[at] = state.astype(BF16)
        piece = got[at].astype(F32)
        decay = piece[8:9, :] + piece[9:10, :]
        state = jnp.exp(decay) * state + piece[:8, :]


def absorb(queries, pieces, most_in, sums_in, most_out, sums_out, final, first=0):
    rows = queries[0].shape[0]
    lane = lax.broadcasted_iota(jnp.int32, (rows, 128), 1)
    row = lax.broadcasted_iota(jnp.int32, (128, 128), 0)
    diagonal = row == lax.broadcasted_iota(jnp.int32, (128, 128), 1)
    scale = QK_DIM**-0.5 * LOG2E
    key = jnp.concatenate([p[:, :128] for p in pieces], axis=0)
    val = jnp.concatenate([p[:, 128:] for p in pieces], axis=0)
    val = jnp.concatenate([val, jnp.ones(val.shape, BF16)], axis=1)
    for s, query in enumerate(queries):
        none = jnp.zeros_like(query)
        both = jnp.concatenate(
            [jnp.where(lane < QK_DIM, query, none), jnp.where(lane < QK_DIM, none, query)],
            axis=0,
        )
        score = dot_nt(both, key)
        most = jnp.max(score, axis=1, keepdims=True)
        if most_in is not None:
            old = most_in[first + s][:, :1]
            most = jnp.maximum(most, old)
        weight = jnp.exp2((score - most) * scale).astype(BF16)
        sums = dot(weight, val)
        if most_in is not None:
            sums = sums + jnp.exp2((old - most) * scale) * sums_in[first + s]
        if final is None:
            most_out[s] = jnp.broadcast_to(most, (2 * rows, 128))
            sums_out[s] = sums
            continue
        out = final[s]
        norm = sums[:, 128:]
        out[: 2 * rows, :] = (sums[:, :128] / norm).astype(BF16)
        level = most * scale + jnp.log2(norm)
        lines = [
            jnp.sum(jnp.where(diagonal, level[m * 128 : (m + 1) * 128], 0.0), 0, keepdims=True)
            for m in range(2 * rows // 128)
        ]
        line = jnp.concatenate(lines, axis=0)
        high = line.astype(BF16).astype(F32)
        middle = (line - high).astype(BF16).astype(F32)
        low = line - high - middle
        fill = jnp.zeros((4, 128), F32)
        tail = jnp.concatenate([high, middle, low, fill], axis=0)
        out[2 * rows : 2 * rows + 16, :] = tail.astype(BF16)


def halves(both):
    rows = both.shape[0] // 2
    return both[:rows], both[rows:]


def absorb_first(near, far, *refs):
    most_out, sums_out = refs[-2:]
    queries = halves(near) + halves(far)
    absorb(queries, refs[:-2], None, None, most_out, sums_out, None)


def absorb_last(first, both, most_in, sums_in, *refs):
    absorb(halves(both), refs[:-2], most_in, sums_in, None, None, refs[-2:], first)


def finish_heads(tags, p0, p1, p2, p3, lam, gain_a, kept, states, gain_r, keep, give):
    core = tags[0]
    parts = (p0, p1, p2, p3)
    row = lax.broadcasted_iota(jnp.int32, (128, 128), 0)
    diagonal = row == lax.broadcasted_iota(jnp.int32, (128, 128), 1)
    results = []
    ending = [states[d * 16 : d * 16 + 16].astype(F32).reshape(HG_KEY, HG_KEY).astype(BF16)
              for d in range(2)]
    for n in range(2):
        ratio = []
        for m in range(2):
            k = m * 2 + n
            levels = []
            for part in parts:
                tail = part[512:528, :].astype(F32)
                line = tail[k : k + 1] + tail[k + 4 : k + 5] + tail[k + 8 : k + 9]
                levels.append(jnp.sum(jnp.where(diagonal, line, 0.0), axis=1, keepdims=True))
            top = functools.reduce(jnp.maximum, levels)
            shares = [jnp.exp2(v - top) for v in levels]
            norm = functools.reduce(jnp.add, shares)
            at = slice(k * 128, (k + 1) * 128)
            both = functools.reduce(
                jnp.add, [w * part[at, :].astype(F32) for part, w in zip(parts, shares)]
            )
            ratio.append(both / norm)
        diff = ratio[0] - lam[core] * ratio[1]
        mean = jnp.mean(diff * diff, axis=1, keepdims=True)
        attn = (diff * lax.rsqrt(mean + EPSILON) * gain_a[...]).astype(BF16)
        at = slice(n * 128, (n + 1) * 128)
        total = kept[at, :128]
        for d in range(2):
            reach = kept[at, (1 + d) * 128 : (2 + d) * 128].astype(BF16)
            total = total + dot_nt(reach, ending[d])
        mean = jnp.mean(total * total, axis=1, keepdims=True)
        rec = (total * lax.rsqrt(mean + EPSILON) * gain_r[...]).astype(BF16)
        results.append(jnp.concatenate([attn, rec], axis=1))
    keep[...] = jnp.where(core == 0, results[0], results[1])
    give[...] = jnp.where(core == 0, results[1], results[0])


def project_out(tags, keep, got, wa, wr, m0, m1, m2, m3, mixed):
    core = tags[0]
    own = pl.ds(pl.multiple_of(core * 128, 128), 128)
    other = pl.ds(pl.multiple_of((1 - core) * 128, 128), 128)
    result = dot(keep[:, :128], wa[own, :]) + dot(got[:, :128], wa[other, :])
    result = result + dot(keep[:, 128:], wr[own, :]) + dot(got[:, 128:], wr[other, :])
    pieces = mixed.shape[0]
    mixed[...] = result.astype(BF16).reshape(pieces, result.shape[0] // pieces, result.shape[1])
    for n, out in enumerate((m0, m1, m2, m3)):
        out[...] = mixed[tags[1] ^ n]


def add_up(p0, p1, p2, p3, out):
    parts = [part[...].astype(F32) for part in (p0, p1, p2, p3)]
    out[...] = functools.reduce(jnp.add, parts).astype(BF16)


def local(
    tokens,
    norm_gain,
    da_query,
    da_key,
    da_value,
    mix_lambda,
    attn_gain,
    rec_query,
    rec_forget_fwd,
    rec_forget_bwd,
    rec_value,
    gate_gap,
    extra_decay,
    init_state,
    rec_gain,
    out_attn,
    out_rec,
):
    rows, width = tokens.shape
    tags = jnp.stack(
        [lax.axis_index(C), lax.axis_index(Y), lax.axis_index(X), lax.axis_index((Z, X))]
    ).astype(jnp.int32)

    extra = jnp.transpose(extra_decay, (0, 2, 1)).reshape(4, rows)
    toks = {s: shifted(tokens, Y, s) for s in (2, 1, 3)}
    weights = [
        da_key,
        da_value,
        da_query,
        rec_value,
        rec_query,
        rec_forget_fwd,
        rec_forget_bwd,
    ]
    partial, gain, squares = call(
        begin,
        [((rows, 7 * 256), F32), ((4, 1, width), F32), ((rows, 128), F32)],
        [tags, tokens, norm_gain.reshape(4, 1, width), *weights],
        scratch=[
            pltpu.VMEM((rows, width), BF16),
            pltpu.VMEM((7, width, 256), BF16),
            pltpu.SemaphoreType.DMA((9,)),
        ],
        specs=[SMEM] + [HBM] * 9,
        flops=2 * rows * width * 7 * 256,
        mib=53,
    )
    mine, theirs = call(
        project,
        [((rows, 7 * 128), BF16), ((rows + 16, 7 * 128), BF16)],
        [tags, toks[1], toks[2], toks[3], gain, squares, extra, partial, *weights],
        scratch=[
            pltpu.VMEM((7, 3 * width, 256), BF16),
            pltpu.VMEM((rows, 7 * 256), F32),
            pltpu.SemaphoreType.DMA((22,)),
        ],
        specs=[SMEM] + [VMEM] * 6 + [HBM] * 8,
        flops=2 * rows * D * 7 * 256,
        mib=53,
    )
    got = shifted(theirs, C, 1)
    kv, query = call(
        join,
        [((2 * rows, 256), BF16), ((2 * rows, 128), BF16)],
        [tags, mine, got],
        specs=[SMEM, VMEM, VMEM],
    )

    up = shifted(kv, Z, 1)
    down = shifted(kv, Z, 7)
    kept, send = call(
        recurrence_local,
        [((2 * rows, 3 * 128), F32), ((32, 16, 128), BF16)],
        [tags, mine, got, gate_gap, extra],
        specs=[SMEM] + [VMEM] * 4,
        flops=2 * rows * 128 * 128 * 40,
    )
    arrived = lax.all_to_all(send, (Z, X), 0, 0, tiled=True)
    up2 = shifted(up, Z, 1)
    down2 = shifted(down, Z, 7)
    beside = lax.ppermute(query, X, [(i, i ^ 1) for i in range(4)])
    near = call(pair_up, ((4 * rows, 128), BF16), [query, beside])
    queries = [near, swapped(near, X, 2)]
    back = call(
        entering_states,
        ((32, 8, 128), BF16),
        [tags, arrived, init_state.reshape(-1, HG_KEY, HG_KEY)],
        scratch=[pltpu.VMEM((HG_KEY, HG_KEY), F32)],
        specs=[SMEM, VMEM, VMEM],
    )
    up3 = shifted(up2, Z, 1)
    down3 = shifted(down2, Z, 7)
    states = lax.all_to_all(back, (Z, X), 0, 0, tiled=True)
    flops = 4 * 512 * 256 * 2 * 2 * 256
    most, sums = call(
        absorb_first,
        [((4, 4 * rows, 128), F32), ((4, 4 * rows, 256), F32)],
        [*queries, kv, up, down, up2, down2],
        flops=5 * flops,
        mib=16,
    )
    up4 = shifted(up3, Z, 1)
    shape = ((4 * rows + 16, 128), BF16)
    parts2, parts3 = call(
        functools.partial(absorb_last, 2),
        [shape] * 2,
        [queries[1], most, sums, up3, down3, up4],
        flops=3 * flops // 2,
        mib=12,
    )
    parts2 = swapped(parts2, X, 2)
    parts3 = swapped(parts3, X, 3)
    parts0, parts1 = call(
        functools.partial(absorb_last, 0),
        [shape] * 2,
        [queries[0], most, sums, up3, down3, up4],
        flops=3 * flops // 2,
        mib=12,
    )
    parts1 = swapped(parts1, X, 1)
    keep, give = call(
        finish_heads,
        [((rows, 256), BF16)] * 2,
        [tags, parts0, parts1, parts2, parts3, mix_lambda, attn_gain[None], kept, states, rec_gain[None]],
        specs=[SMEM] + [VMEM] * 4 + [SMEM] + [VMEM] * 4,
    )
    got = shifted(give, C, 1)
    blocks = call(
        project_out,
        [((rows // 4, D), BF16)] * 4,
        [tags, keep, got, out_attn, out_rec],
        scratch=[pltpu.VMEM((4, rows // 4, D), BF16)],
        specs=[SMEM] + [VMEM] * 4,
        flops=2 * rows * D * 512,
    )
    two = swapped(blocks[2], Y, 2)
    three = swapped(blocks[3], Y, 3)
    one = swapped(blocks[1], Y, 1)
    return call(add_up, ((rows // 4, D), BF16), [blocks[0], one, two, three])


def solution(mesh):
    torus = Mesh(mesh.devices.reshape(8, 4, 2, mesh.shape["tp"]), (Z, X, C, Y))
    return jax.shard_map(
        local,
        mesh=torus,
        in_specs=(
            P(SP, Y),
            P(),
            P(None, Y),
            P(None, Y),
            P(None, Y),
            P(Y),
            P(),
            P(None, Y),
            P(None, Y),
            P(None, Y),
            P(None, Y),
            P(None, Y),
            P(None, SP, Y),
            P(None, Y, None, None),
            P(),
            P(Y, None),
            P(Y, None),
        ),
        out_specs=P((*SP, Y), None),
        check_vma=False,
    )
```
